512 devices in a mesh: sp: 32 (over z, x), tp: 16 (over y, core).
Axes of the slice: x: 4, y: 8, z: 8, core: 2. Of those that a mesh axis runs over, the one named last changes fastest.
Arguments:
- target_rows: bfloat16 [2048, 2048], P(('sp', 'tp')), may hold values from -6 to 6
- source_rows: bfloat16 [8192, 2048], P(('sp', 'tp')), may hold values from -6 to 6
- norm_gain: bfloat16 [2048], replicated, may hold values from 0.099609375 to 1.8984375
- query_weight: bfloat16 [2048, 4096], P(None, 'tp'), may hold values from -0.125 to 0.125
- key_weight: bfloat16 [2048, 4096], P(None, 'tp'), may hold values from -0.125 to 0.125
- value_weight: bfloat16 [2048, 4096], P(None, 'tp'), may hold values from -0.125 to 0.125
- output_weight: bfloat16 [4096, 2048], P('tp'), may hold values from -0.09375 to 0.09375
- saved_output: bfloat16 [2048, 4096], P('sp', 'tp'), may hold values from -3 to 3
- norm_offset: bfloat16 [2048, 16], P('sp', 'tp'), may hold values from 0.25 to 1.25
- output_grad: bfloat16 [2048, 2048], P(('sp', 'tp')), may hold values from -192 to 192
Outputs:
- target_grad: float32 [2048, 2048], P(('sp', 'tp'))
- source_grad: float32 [8192, 2048], P(('sp', 'tp'))
- query_weight_grad: float32 [2048, 4096], P('sp', 'tp')
The draws below stay inside these ranges and needn't reach their ends.
All inputs are finite; a program needn't handle non-finite values.
Results may differ from the reference program's by a relative error of at most 0.033.
Values may be sent and summed in bfloat16 or wider, within the bound.
A program may use at most 64 MiB of HBM per device.

```python
import math
import jax
import jax.numpy as jnp
from jax import lax

D = 2048
HEADS = 16
HEAD_DIM = 256
TARGET = 2048
SOURCE = 8192


def block_scale(rng, dims, pieces, low, top_value):
    def one(axis_at, shards_of):
        steps = jax.random.uniform(jax.random.fold_in(jax.random.fold_in(rng, 6), axis_at), (shards_of,), jnp.float32, low / len(pieces), top_value / len(pieces))
        return jnp.repeat(jnp.exp(steps), dims[axis_at] // shards_of).reshape((-1,) + (1,) * (len(dims) - axis_at - 1))

    factor_of = one(*pieces[0])
    for cut in pieces[1:]:
        factor_of = factor_of * one(*cut)
    return factor_of


def bell_draw(key, extent, scale, bound, cuts=(), kind=jnp.bfloat16):
    values = jax.random.normal(key, extent, jnp.float32) * scale
    if len(cuts) > 0:
        values = block_scale(key, extent, cuts, -0.22, 0.18) * values
    return jnp.clip(values, min=-bound, max=bound).astype(kind)


def setup_inputs(seed: int = 0) -> dict:
    streams_of = jax.random.split(jax.random.key(seed), 11)
    target_rows = bell_draw(streams_of[0], (TARGET, D), 1.0, 6.0, ((0, 512),))
    source_rows = bell_draw(streams_of[1], (SOURCE, D), 1.0, 6.0, ((0, 512),))
    norm_gain = jnp.clip(1.0 + 0.18 * jax.random.normal(streams_of[2], (D,), jnp.float32), 0.099609375, 1.8984375).astype(jnp.bfloat16)
    query_weight = bell_draw(streams_of[3], (D, HEADS * HEAD_DIM), D ** -0.5, 0.125, ((1, 16),))
    key_weight = bell_draw(streams_of[4], (D, HEADS * HEAD_DIM), D ** -0.5, 0.125, ((1, 16),))
    value_weight = bell_draw(streams_of[5], (D, HEADS * HEAD_DIM), D ** -0.5, 0.125, ((1, 16),))
    output_weight = bell_draw(streams_of[6], (HEADS * HEAD_DIM, D), (HEADS * HEAD_DIM) ** -0.5, 0.09375, ((0, 16),))
    saved_output = bell_draw(streams_of[7], (TARGET, HEADS * HEAD_DIM), 0.5, 3.0, ((0, 32), (1, 16)))
    norm_offset = jnp.clip(0.25 + 1.0 * jax.random.uniform(streams_of[8], (TARGET, HEADS), jnp.float32) ** block_scale(streams_of[8], (TARGET, HEADS), ((0, 32), (1, 16)), -0.2, 0.2), 0.25, 1.25).astype(jnp.bfloat16)
    output_grad = bell_draw(streams_of[9], (TARGET, D), 32.0, 192.0, ((0, 512),))
    return {"target_rows": target_rows, "source_rows": source_rows, "norm_gain": norm_gain, "query_weight": query_weight, "key_weight": key_weight, "value_weight": value_weight, "output_weight": output_weight, "saved_output": saved_output, "norm_offset": norm_offset, "output_grad": output_grad}


EPSILON = 1e-06

def head_grads(operands):
    query_rows, head_gradient, shifts, deltas, key_row_block, value_row_block = operands
    score_scale = HEAD_DIM ** (-0.5)
    score_matrix = jnp.dot(query_rows, key_row_block.T, preferred_element_type=jnp.float32)
    prob_rows = jnp.exp(score_matrix * score_scale - shifts[:, None])
    prob_grad = jnp.dot(head_gradient, value_row_block.T, preferred_element_type=jnp.float32)
    score_grad = prob_rows * (prob_grad - deltas.astype(jnp.float32)[:, None]) * score_scale
    probability_rounded = prob_rows.astype(jnp.bfloat16)
    score_rounded = score_grad.astype(jnp.bfloat16)
    query_grad = jnp.dot(score_rounded, key_row_block, preferred_element_type=jnp.float32)
    key_grad = jnp.dot(score_rounded.T, query_rows, preferred_element_type=jnp.float32)
    value_grad = jnp.dot(probability_rounded.T, head_gradient, preferred_element_type=jnp.float32)
    return (query_grad, key_grad, value_grad)

def by_head(array, row_count):
    return array.reshape(row_count, HEADS, HEAD_DIM).transpose(1, 0, 2)

def from_head(array, row_count):
    return array.transpose(1, 0, 2).reshape(row_count, HEADS * HEAD_DIM)

def reference(target_rows, source_rows, norm_gain, query_weight, key_weight, value_weight, output_weight, saved_output, norm_offset, output_grad):
    target_float = target_rows.astype(jnp.float32)
    gain_float = norm_gain.astype(jnp.float32)
    inverse = lax.rsqrt(lax.optimization_barrier(jnp.mean(target_float * target_float, axis=1, keepdims=True)) + EPSILON)
    normed = (target_float * inverse * gain_float).astype(jnp.bfloat16)
    query_rows = jnp.dot(normed, query_weight, preferred_element_type=jnp.float32).astype(jnp.bfloat16)
    key_row_block = jnp.dot(source_rows, key_weight, preferred_element_type=jnp.float32).astype(jnp.bfloat16)
    value_row_block = jnp.dot(source_rows, value_weight, preferred_element_type=jnp.float32).astype(jnp.bfloat16)
    head_gradient = jnp.dot(output_grad, output_weight.T, preferred_element_type=jnp.float32).astype(jnp.bfloat16)
    products = head_gradient.astype(jnp.float32) * saved_output.astype(jnp.float32)
    deltas = lax.optimization_barrier(jnp.sum(products.reshape(TARGET, HEADS, HEAD_DIM), axis=2)).astype(jnp.bfloat16)
    shifts = (math.log(SOURCE) + norm_offset.astype(jnp.float32)).T
    outputs = lax.map(head_grads, (by_head(query_rows, TARGET), by_head(head_gradient, TARGET), shifts, deltas.T, by_head(key_row_block, SOURCE), by_head(value_row_block, SOURCE)))
    query_flat = from_head(outputs[0].astype(jnp.bfloat16), TARGET)
    key_flat = from_head(outputs[1].astype(jnp.bfloat16), SOURCE)
    value_flat = from_head(outputs[2].astype(jnp.bfloat16), SOURCE)
    normed_grad = jnp.dot(query_flat, query_weight.T, preferred_element_type=jnp.float32)
    scaled = normed_grad * gain_float
    target_grad = inverse * scaled - target_float * inverse ** 3 * lax.optimization_barrier(jnp.mean(scaled * target_float, axis=1, keepdims=True))
    source_grad = jnp.dot(key_flat, key_weight.T, preferred_element_type=jnp.float32) + jnp.dot(value_flat, value_weight.T, preferred_element_type=jnp.float32)
    weight_grad = jnp.dot(normed.T, query_flat, preferred_element_type=jnp.float32)
    return (target_grad, source_grad, weight_grad)
```

```python
import math

import jax
import jax.numpy as jnp
from jax import lax
from jax.experimental import pallas as pl
from jax.experimental.pallas import tpu as pltpu
from jax.sharding import Mesh
from jax.sharding import PartitionSpec as P

SP = ("sp_0", "sp_1")
SP_TP = ("sp_0", "sp_1", "tp")
EPSILON = 1e-06
SCALE = 256 ** (-0.5)
SHIFT = math.log(8192)
MESH = pl.DeviceIdType.MESH
F32 = jnp.float32
BF16 = jnp.bfloat16
NZ, NX, NY = 8, 4, 8

SENDS, RECVS = 256, 256


def nt(left, right):
    return lax.dot_general(left, right, (((1,), (1,)), ((), ())), preferred_element_type=F32)


def nn(left, right):
    return lax.dot_general(left, right, (((1,), (0,)), ((), ())), preferred_element_type=F32)


def kernel(
    tr_ref, sr_ref, gain_ref, wq_hbm, wk_hbm, wv_hbm, wo_hbm, saved_ref, off_ref, og_ref,
    tgrad_ref, sgrad_ref, wgrad_ref,
    tg, xn, xo, xnt, sg, wq, wk, wv, wo, zf, xf, kb, vb, dk, dv,
    part1, reli1, relo1, xin1, zout1, zin1,
    part2, reli2, relo2, xin2, zout2, zin2,
    gout, gin, gsum, grecv, nout, nin, nsum, nrecv,
    ssem, rsem, wsem,
):
    z = lax.axis_index("sp_0")
    x = lax.axis_index("sp_1")
    t = lax.axis_index("tp")
    y = t // 2
    c = t % 2
    way = 1 - 2 * c

    def zat(k):
        return ((z + k) % NZ, x, t)

    def xat(k):
        return (z, (x + k) % NX, t)

    def yat(k):
        return (z, x, ((y + k) % NY) * 2 + c)

    mate = (z, x, t + way)
    ids = {"s": 0}
    names = {}
    pending = []

    def slot_of(name):
        if name not in names:
            names[name] = len(names)
        return names[name]

    def send(src, dst, name, dev):
        k = ids["s"]
        ids["s"] = k + 1
        copy = pltpu.make_async_remote_copy(
            src_ref=src, dst_ref=dst, send_sem=ssem.at[k], recv_sem=rsem.at[slot_of(name)],
            device_id=dev, device_id_type=MESH,
        )
        copy.start()
        pending.append(copy)

    def wait(dst, name):
        pltpu.make_async_remote_copy(
            src_ref=dst, dst_ref=dst, send_sem=ssem.at[0], recv_sem=rsem.at[slot_of(name)],
            device_id=mate, device_id_type=MESH,
        ).wait_recv()

    weights = {}
    for k, (name, src, dst) in enumerate(
        (("q", wq_hbm, wq), ("o", wo_hbm, wo), ("k", wk_hbm, wk), ("v", wv_hbm, wv))
    ):
        weights[name] = pltpu.make_async_copy(src, dst, wsem.at[k])
        weights[name].start()

    barrier = pltpu.get_barrier_semaphore()
    peers = [mate] + [yat(k) for k in range(1, NY)] + [xat(1), xat(3)] + [zat(k) for k in range(1, NZ)]
    for dev in peers:
        pl.semaphore_signal(barrier, inc=1, device_id=dev, device_id_type=MESH)

    gain = gain_ref[...].astype(F32)
    target = tr_ref[...].astype(F32)
    inverse = lax.rsqrt(jnp.mean(target * target, axis=1, keepdims=True) + EPSILON)
    tg[t] = jnp.concatenate(
        [target * inverse * gain, og_ref[...].astype(F32)], axis=0
    ).astype(BF16)
    sg[0] = sr_ref[...]
    pl.semaphore_wait(barrier, len(peers))

    def tg_of(k):
        return tg.at[((y + NY - k) % NY) * 2 + c]

    def tg_mate(k):
        return tg.at[((y + NY - k) % NY) * 2 + 1 - c]

    for k in (3, 5, 2, 6, 1, 7):
        send(tg_of(0), tg_of(0), ("tg", k), yat(k))
    send(tg_of(0), tg_of(0), ("tgm", 0), mate)
    for k in (3, 5, 2, 6, 1, 7):
        send(sr_ref, sg.at[k], ("sg", k), yat(k))
    send(sr_ref, sg.at[8], ("sgm", 0), mate)

    for k in (1, 7, 2, 6, 3, 5):
        wait(tg_of(k), ("tg", k))
        send(tg_of(k), tg_of(k), ("tgm", k), mate)
    relay = tg.at[((y + NY - 3 * way) % NY) * 2 + c]
    send(relay, relay, ("tg", 4), (z, x, ((y + NY + way) % NY) * 2 + c))
    wait(tg_of(4), ("tg", 4))
    send(tg_of(4), tg_of(4), ("tgm", 4), mate)
    for k in (0, 1, 7, 2, 6, 3, 5, 4):
        wait(tg_mate(k), ("tgm", k))

    for s in range(16):
        rows = tg[s].astype(F32)
        xn[4 * s : 4 * s + 4] = rows[0:4]
        xo[4 * s : 4 * s + 4] = rows[4:8]
    weights["q"].wait()
    queries = nn(xn[...].astype(BF16), wq[...]).astype(BF16)
    zf[0, x, 0:64] = queries
    weights["o"].wait()
    hgrad = nt(xo[...].astype(BF16), wo[...]).astype(BF16)
    xf[0, x] = hgrad
    deltas = jnp.sum(hgrad.astype(F32) * saved_ref[...].astype(F32), axis=1, keepdims=True)
    lane = lax.broadcasted_iota(jnp.int32, (64, 128), 1)
    both = jnp.where(lane == 0, off_ref[...].astype(F32), jnp.where(lane == 1, deltas, 0.0))
    place = lax.broadcasted_iota(jnp.int32, (64, 256), 1) == x * 64 + lax.broadcasted_iota(
        jnp.int32, (64, 256), 0
    )
    stats = nn(both.T.astype(BF16), place.astype(F32).astype(BF16))
    zf[0, x, 64:80] = stats[0:16].astype(BF16)

    def xs(e):
        return (x + NX - e) % NX

    def zf_x(k):
        send(zf.at[k, x], zf.at[k, x], ("zfx", k, 1), xat(1))
        send(zf.at[k, x], zf.at[k, x], ("zfx", k, 3), xat(3))

    def zf_z(k):
        if k:
            wait(zf.at[k, x], ("zfz", k))
        if k <= 3:
            send(zf.at[k, x], zf.at[k + 1, x], ("zfz", k + 1), zat(1))
        if k == 0 or k >= 6:
            send(zf.at[k, x], zf.at[(k - 1) % NZ, x], ("zfz", (k - 1) % NZ), zat(7))

    def zf_relay(k):
        wait(zf.at[k, xs(1)], ("zfx", k, 1))
        wait(zf.at[k, xs(3)], ("zfx", k, 3))
        e = 1 if k % 2 == 0 else 3
        send(zf.at[k, xs(e)], zf.at[k, xs(e)], ("zfx", k, 2), xat(e))

    def zf_end(k):
        wait(zf.at[k, xs(2)], ("zfx", k, 2))

    def xf_z(k, e):
        if k:
            wait(xf.at[k, xs(e)], ("xfz", k, e))
        if k <= 2:
            send(xf.at[k, xs(e)], xf.at[k + 1, xs(e)], ("xfz", k + 1, e), zat(1))
        if k == 0 or k >= 5:
            send(xf.at[k, xs(e)], xf.at[(k - 1) % NZ, xs(e)], ("xfz", (k - 1) % NZ, e), zat(7))

    def sg_in(k):
        wait(sg.at[k], ("sg", k))
        send(sg.at[k], sg.at[8 + k], ("sgm", k), mate)

    send(xf.at[0, x], xf.at[0, x], ("xfx", 1), xat(1))
    send(xf.at[0, x], xf.at[0, x], ("xfx", 3), xat(3))
    zf_z(0)
    xf_z(0, 0)
    zf_x(0)

    sg_in(1)
    sg_in(7)
    wait(xf.at[0, xs(1)], ("xfx", 1))
    xf_z(0, 1)
    wait(xf.at[0, xs(3)], ("xfx", 3))
    send(xf.at[0, xs(3)], xf.at[0, xs(3)], ("xfx", 2), xat(3))
    xf_z(0, 3)
    zf_z(1)
    zf_z(7)
    zf_x(1)
    zf_x(7)
    zf_relay(0)
    wait(xf.at[0, xs(2)], ("xfx", 2))
    xf_z(0, 2)
    sg_in(2)
    sg_in(6)
    for e in range(4):
        xf_z(1, e)
        xf_z(7, e)
    zf_z(2)
    zf_z(6)
    zf_x(2)
    zf_x(6)
    zf_relay(1)
    zf_relay(7)
    sg_in(3)
    sg_in(5)
    far = 3 + 2 * c
    send(sg.at[far], sg.at[4], ("sg", 4), (z, x, ((y + NY + way) % NY) * 2 + c))
    for f in range(4):
        xnt[2 * f] = jnp.transpose(xn[:, 512 * f : 512 * f + 256]).astype(BF16)
        xnt[2 * f + 1] = jnp.transpose(xn[:, 512 * f + 256 : 512 * f + 512]).astype(BF16)
    for e in range(4):
        xf_z(2, e)
        xf_z(6, e)
    zf_z(3)
    zf_z(5)
    zf_x(3)
    zf_x(5)
    zf_relay(2)
    zf_relay(6)
    sg_in(4)
    for e in range(4):
        xf_z(3, e)
        xf_z(5, e)
    zf_z(4)
    zf_x(4)
    zf_relay(3)
    zf_relay(5)
    for k in range(8):
        wait(sg.at[8 + k], ("sgm", k))
    rows = sg[...].reshape(256, 2048)
    weights["k"].wait()
    kb[...] = nn(rows, wk[...]).astype(BF16)
    zf_relay(4)
    weights["v"].wait()
    vb[...] = nn(rows, wv[...]).astype(BF16)

    def x_sends(tag, k, part, reli, xin):
        e = 1 if k % 2 == 0 else 3
        send(part.at[k, (x + 2) % NX], reli.at[k], (tag, "rel", k), xat(e))
        send(part.at[k, (x + 4 - e) % NX], xin.at[k, 1], (tag, "x1", k), xat(4 - e))

    def x_relay(tag, k, part, reli, relo, xin):
        e = 1 if k % 2 == 0 else 3
        wait(reli.at[k], (tag, "rel", k))
        relo[k] = (part[k, (x + e) % NX].astype(F32) + reli[k].astype(F32)).astype(BF16)
        send(relo.at[k], xin.at[k, 0], (tag, "x0", k), xat(e))

    def x_sum(tag, k, part, xin):
        wait(xin.at[k, 0], (tag, "x0", k))
        wait(xin.at[k, 1], (tag, "x1", k))
        return part[k, x].astype(F32) + xin[k, 0].astype(F32) + xin[k, 1].astype(F32)

    def z_send(tag, k, part, xin, zout, zin):
        zout[k] = x_sum(tag, k, part, xin).astype(BF16)
        send(zout.at[k], zin.at[k], (tag, "z", k), zat(NZ - k))

    def z_sum(tag, part, xin, zin):
        total = x_sum(tag, 0, part, xin)
        for k in range(1, NZ):
            wait(zin.at[k], (tag, "z", k))
            total += zin[k].astype(F32)
        return total

    def group(k, first):
        q = zf[k, :, 0:64, :].reshape(256, 256)
        h = xf[k].reshape(256, 256)
        stat = jnp.sum(zf[k, :, 64:80, :].astype(F32), axis=0)
        score = nt(kb[...], q)
        prob = jnp.exp(score * SCALE - (SHIFT + stat[0:1]))
        grad = prob * (nt(vb[...], h) - stat[1:2]) * SCALE
        prob = prob.astype(BF16)
        dv_new = nn(prob, h)
        dk_new = nn(grad.astype(BF16), q)
        if first:
            dv[...] = dv_new
            dk[...] = dk_new
        else:
            dv[...] += dv_new
            dk[...] += dk_new
        dq = nn(jnp.transpose(grad).astype(BF16), kb[...])
        part1[k] = dq.astype(BF16).reshape(4, 64, 256)

    for e in range(4):
        xf_z(4, e)
    order = (1, 7, 2, 6, 3, 5, 4, 0)
    one = (part1, reli1)
    for n, k in enumerate(order):
        zf_end(k)
        group(k, n == 0)
        x_sends("q", k, part1, reli1, xin1)
        if n >= 1:
            x_relay("q", order[n - 1], part1, reli1, relo1, xin1)
        if n >= 2:
            z_send("q", order[n - 2], part1, xin1, zout1, zin1)
    x_relay("q", 0, part1, reli1, relo1, xin1)
    z_send("q", 4, part1, xin1, zout1, zin1)

    dkb = dk[...].astype(BF16)
    dvb = dv[...].astype(BF16)
    for half in (1, 0):
        for f in range(4):
            cols = pl.ds(512 * f, 512)
            lo = 128 * half
            gout[half, :, :, cols] = (
                (nt(dkb[lo : lo + 128], wk[cols, :]) + nt(dvb[lo : lo + 128], wv[cols, :]))
                .astype(BF16)
                .reshape(8, 16, 512)
            )
        if half:
            send(gout.at[1], gin, ("gm",), mate)
    wait(gin, ("gm",))
    for k in (4, 3, 5, 2, 6, 1, 7):
        gsum[k] = (gout[0, k].astype(F32) + gin[k].astype(F32)).astype(BF16)
        send(gsum.at[k], grecv.at[k], ("g", k), yat(NY - k))

    qflat = z_sum("q", part1, xin1, zin1).astype(BF16)

    def weight_part(k):
        part2[k] = nn(xnt[(z + NZ - k) % NZ], qflat).astype(BF16).reshape(4, 64, 256)

    for n, k in enumerate(order):
        weight_part(k)
        x_sends("w", k, part2, reli2, xin2)
        if n >= 2:
            x_relay("w", order[n - 2], part2, reli2, relo2, xin2)

    for f in range(2):
        halves = [nt(qflat, wq[1024 * g + 512 * f : 1024 * g + 512 * f + 512, :]) for g in range(2)]
        for s in range(16):
            nout[s % 2, s // 2, :, 512 * f : 512 * f + 512] = jnp.concatenate(
                [part[4 * s : 4 * s + 4] for part in halves], axis=0
            ).astype(BF16)
    send(nout.at[1 - c], nin, ("nm",), mate)
    x_relay("w", 4, part2, reli2, relo2, xin2)
    x_relay("w", 0, part2, reli2, relo2, xin2)
    wait(nin, ("nm",))
    nsum[...] = (nout[c].astype(F32) + nin[...].astype(F32)).astype(BF16)
    for k in (4, 3, 5, 2, 6, 1, 7):
        send(nsum.at[(y + NY - k) % NY], nrecv.at[k], ("n", k), yat(NY - k))
    for k in order[:-1]:
        z_send("w", k, part2, xin2, zout2, zin2)

    total = gout[0, 0].astype(F32) + gin[0].astype(F32)
    for k in (1, 7, 2, 6, 3, 5, 4):
        wait(grecv.at[k], ("g", k))
        total += grecv[k].astype(F32)
    sgrad_ref[...] = total

    total = nsum[y].astype(F32)
    for k in (1, 7, 2, 6, 3, 5, 4):
        wait(nrecv.at[k], ("n", k))
        total += nrecv[k].astype(F32)
    scaled = jnp.concatenate([total[0:4], total[4:8]], axis=1) * gain
    mean = jnp.mean(scaled * target, axis=1, keepdims=True)
    tgrad_ref[...] = inverse * scaled - target * (inverse * inverse * inverse) * mean

    wgrad_ref[...] = z_sum("w", part2, xin2, zin2)

    for copy in pending:
        copy.wait_send()
    assert ids["s"] <= SENDS and len(names) <= RECVS


def body(tr, sr, gain, wq, wk, wv, wo, saved, offset, og):
    vm = pl.BlockSpec(memory_space=pltpu.VMEM)
    hb = pl.BlockSpec(memory_space=pl.ANY)

    def buf(*shape, dtype=BF16):
        return pltpu.VMEM(shape, dtype)

    reduce_bufs = [
        buf(8, 4, 64, 256), buf(8, 64, 256), buf(8, 64, 256), buf(8, 2, 64, 256),
        buf(8, 64, 256), buf(8, 64, 256),
    ]
    return pl.pallas_call(
        kernel,
        out_shape=(
            jax.ShapeDtypeStruct((4, 2048), F32),
            jax.ShapeDtypeStruct((16, 2048), F32),
            jax.ShapeDtypeStruct((64, 256), F32),
        ),
        in_specs=[vm, vm, vm, hb, hb, hb, hb, vm, vm, vm],
        out_specs=(vm, vm, vm),
        scratch_shapes=[
            buf(16, 8, 2048), buf(64, 2048, dtype=F32), buf(64, 2048, dtype=F32),
            buf(8, 256, 64), buf(16, 16, 2048),
            buf(2048, 256), buf(2048, 256), buf(2048, 256), buf(256, 2048),
            buf(8, 4, 80, 256), buf(8, 4, 64, 256),
            buf(256, 256), buf(256, 256),
            buf(256, 256, dtype=F32), buf(256, 256, dtype=F32),
            *reduce_bufs, *reduce_bufs,
            buf(2, 8, 16, 2048), buf(8, 16, 2048), buf(8, 16, 2048), buf(8, 16, 2048),
            buf(2, 8, 8, 1024), buf(8, 8, 1024), buf(8, 8, 1024), buf(8, 8, 1024),
            pltpu.SemaphoreType.DMA((SENDS,)),
            pltpu.SemaphoreType.DMA((RECVS,)),
            pltpu.SemaphoreType.DMA((4,)),
        ],
        compiler_params=pltpu.CompilerParams(
            collective_id=0, has_side_effects=True, vmem_limit_bytes=60 * 1024 * 1024
        ),
    )(tr, sr, gain.reshape(1, 2048), wq, wk, wv, wo, saved, offset, og)


def solution(mesh):
    split = Mesh(mesh.devices.reshape(NZ, NX, mesh.shape["tp"]), ("sp_0", "sp_1", "tp"))
    placed = (
        P(SP_TP, None), P(SP_TP, None), P(), P(None, "tp"), P(None, "tp"), P(None, "tp"),
        P("tp", None), P(SP, "tp"), P(SP, "tp"), P(SP_TP, None),
    )
    return jax.shard_map(
        body,
        mesh=split,
        in_specs=placed,
        out_specs=(P(SP_TP, None), P(SP_TP, None), P(SP, "tp")),
        check_vma=False,
    )
```

```python
import math

import jax
import jax.numpy as jnp
from jax import lax
from jax.experimental import pallas as pl
from jax.experimental.pallas import tpu as pltpu
from jax.sharding import Mesh
from jax.sharding import PartitionSpec as P

SP = ("sp_0", "sp_1")
SP_TP = ("sp_0", "sp_1", "tp")
EPSILON = 1e-06
SCALE = 256 ** (-0.5)
SHIFT = math.log(8192)
MESH = pl.DeviceIdType.MESH
F32 = jnp.float32
BF16 = jnp.bfloat16
NZ, NX, NY = 8, 4, 8
UNIT = 8192
UNITS = 1024
RECVS = 112


def nt(left, right):
    return lax.dot_general(left, right, (((1,), (1,)), ((), ())), preferred_element_type=F32)


def nn(left, right):
    return lax.dot_general(left, right, (((1,), (0,)), ((), ())), preferred_element_type=F32)


def kernel(
    tr_hbm, sr_hbm, gain_hbm, wq_hbm, wk_hbm, wv_hbm, wo_hbm, saved_hbm, off_hbm, og_hbm,
    tgrad_ref, sgrad_ref, wgrad_ref,
    tr, gn, sv, of, og,
    tg, xn, xo, nb, nr, nrt, sg, wq, wk, wv, wo, zf, xf, kb, vb, dk, dv,
    part, reli, relo, xin, zout, zin,
    qz, wpart, win,
    gout, gin, gsum, grecv, nout, nin, nsum, nrecv,
    units, ssem, rsem, lsem,
):
    z = lax.axis_index("sp_0")
    x = lax.axis_index("sp_1")
    t = lax.axis_index("tp")
    y = t // 2
    c = t % 2
    way = 1 - 2 * c

    def zat(k):
        return ((z + k) % NZ, x, t)

    def xat(k):
        return (z, (x + k) % NX, t)

    def yat(k):
        return (z, x, ((y + k) % NY) * 2 + c)

    mate = (z, x, t + way)
    names = {}
    sent = [0]
    scope = [None]

    def phase(name):
        if scope[0] is not None:
            scope[0].__exit__(None, None, None)
        scope[0] = jax.named_scope(name) if name else None
        if name:
            scope[0].__enter__()

    def size(ref):
        return math.prod(ref.shape) * 2

    def slot_of(name):
        if name not in names:
            names[name] = len(names)
        return names[name]

    def send(src, dst, name, dev):
        assert size(src) % UNIT == 0
        sent[0] += size(src) // UNIT
        pltpu.make_async_remote_copy(
            src_ref=src, dst_ref=dst, send_sem=ssem.at[0], recv_sem=rsem.at[slot_of(name)],
            device_id=dev, device_id_type=MESH,
        ).start()

    def wait(dst, name):
        pltpu.make_async_remote_copy(
            src_ref=dst, dst_ref=dst, send_sem=ssem.at[0], recv_sem=rsem.at[slot_of(name)],
            device_id=mate, device_id_type=MESH,
        ).wait_recv()

    phase("start")
    loads = {}
    for k, (name, src, dst) in enumerate(
        (
            ("tr", tr_hbm, tr), ("og", og_hbm, og), ("gn", gain_hbm, gn), ("sr", sr_hbm, sg.at[0]),
            ("of", off_hbm, of), ("sv", saved_hbm, sv),
            ("q", wq_hbm, wq), ("o", wo_hbm, wo), ("k", wk_hbm, wk), ("v", wv_hbm, wv),
        )
    ):
        loads[name] = pltpu.make_async_copy(src, dst, lsem.at[k])
        loads[name].start()

    barrier = pltpu.get_barrier_semaphore()
    peers = [mate] + [yat(k) for k in range(1, NY)] + [xat(k) for k in range(1, NX)]
    peers += [zat(k) for k in range(1, NZ)]
    for dev in peers:
        pl.semaphore_signal(barrier, inc=1, device_id=dev, device_id_type=MESH)

    for name in ("tr", "og", "gn"):
        loads[name].wait()
    gain = gn[...].astype(F32)
    gain = jnp.concatenate([gain[s : s + 1] for s in range(16)], axis=1)
    target = tr[...].astype(F32)
    inverse = lax.rsqrt(jnp.mean(target * target, axis=1, keepdims=True) + EPSILON)
    tg[c, y] = jnp.concatenate(
        [target * inverse * gain, og[...].astype(F32)], axis=0
    ).astype(BF16)
    phase("barrier")
    pl.semaphore_wait(barrier, len(peers))

    phase("tgwait")

    def tg_of(k):
        return tg.at[c, (y + NY - k) % NY]

    for k in (4, 3, 5, 2, 6, 1, 7):
        send(tg_of(0), tg_of(0), ("tg", k), yat(k))
    send(tg_of(0), tg_of(0), ("tgm",), mate)
    for k in (1, 7, 2, 6, 3, 5, 4):
        wait(tg_of(k), ("tg", k))
        send(tg_of(k), tg_of(k), ("tgm",), mate)
    loads["sr"].wait()
    for k in (3, 5, 2, 6, 1, 7):
        send(sg.at[0], sg.at[k], ("sg", k), yat(k))
    send(sg.at[0], sg.at[8], ("sgm",), mate)
    phase("tgmate")
    wait(tg.at[1 - c], ("tgm",))

    phase("qproj")
    for s in range(16):
        rows = tg[s % 2, s // 2].astype(F32)
        xn[4 * s : 4 * s + 4] = rows[0:4]
        xo[4 * s : 4 * s + 4] = rows[4:8]
    loads["q"].wait()
    queries = nn(xn[...].astype(BF16), wq[...]).astype(BF16)
    zf[0, x, 0:64] = queries
    loads["o"].wait()
    hgrad = nt(xo[...].astype(BF16), wo[...]).astype(BF16)
    xf[0, x] = hgrad
    loads["sv"].wait()
    loads["of"].wait()
    deltas = jnp.sum(hgrad.astype(F32) * sv[...].astype(F32), axis=1, keepdims=True)
    deltas = jnp.broadcast_to(deltas, (64, 128)).T[0:16]
    first = lax.broadcasted_iota(jnp.int32, (16, 64), 0) == 0
    both = jnp.where(first, of[...].astype(F32), deltas).astype(BF16)
    place = lax.broadcasted_iota(jnp.int32, (64, 256), 1) == x * 64 + lax.broadcasted_iota(
        jnp.int32, (64, 256), 0
    )
    zf[0, x, 64:80] = nn(both, place.astype(F32).astype(BF16)).astype(BF16)

    def xs(e):
        return (x + NX - e) % NX

    def zf_x(k):
        send(zf.at[k, x], zf.at[k, x], ("zfx", k, 1), xat(1))
        send(zf.at[k, x], zf.at[k, x], ("zfx", k, 3), xat(3))

    def zf_z(k):
        if k:
            wait(zf.at[k, x], ("zfz", k))
        if k <= 3:
            send(zf.at[k, x], zf.at[k + 1, x], ("zfz", k + 1), zat(1))
        if k == 0 or k >= 6:
            send(zf.at[k, x], zf.at[(k - 1) % NZ, x], ("zfz", (k - 1) % NZ), zat(7))

    def zf_relay(k):
        wait(zf.at[k, xs(1)], ("zfx", k, 1))
        wait(zf.at[k, xs(3)], ("zfx", k, 3))
        e = 1 if k % 2 == 0 else 3
        send(zf.at[k, xs(e)], zf.at[k, xs(e)], ("zfx", k, 2), xat(e))

    def zf_end(k):
        wait(zf.at[k, xs(2)], ("zfx", k, 2))

    def xf_z(k, e):
        if k:
            wait(xf.at[k, xs(e)], ("xfz", k, e))
        if k <= 2:
            send(xf.at[k, xs(e)], xf.at[k + 1, xs(e)], ("xfz", k + 1, e), zat(1))
        if k == 0 or k >= 5:
            send(xf.at[k, xs(e)], xf.at[(k - 1) % NZ, xs(e)], ("xfz", (k - 1) % NZ, e), zat(7))

    def sg_in(k):
        wait(sg.at[k], ("sg", k))
        send(sg.at[k], sg.at[8 + k], ("sgm",), mate)

    phase("spsend")
    send(xf.at[0, x], xf.at[0, x], ("xfx", 1), xat(1))
    send(xf.at[0, x], xf.at[0, x], ("xfx", 3), xat(3))
    zf_z(0)
    xf_z(0, 0)
    zf_x(0)

    phase("step1")
    for f in range(8):
        nb[f] = xn[:, 256 * f : 256 * f + 256].astype(BF16)
    wait(xf.at[0, xs(1)], ("xfx", 1))
    xf_z(0, 1)
    wait(xf.at[0, xs(3)], ("xfx", 3))
    send(xf.at[0, xs(3)], xf.at[0, xs(3)], ("xfx", 2), xat(3))
    xf_z(0, 3)
    zf_z(1)
    zf_z(7)
    zf_x(1)
    zf_x(7)
    zf_relay(0)
    sg_in(1)
    sg_in(7)
    wait(xf.at[0, xs(2)], ("xfx", 2))
    xf_z(0, 2)
    phase("step2")
    for e in (0, 1, 3, 2):
        xf_z(1, e)
        xf_z(7, e)
    zf_z(2)
    zf_z(6)
    zf_x(2)
    zf_x(6)
    sg_in(2)
    sg_in(6)
    zf_relay(1)
    zf_relay(7)
    phase("step3")
    for e in (0, 1, 3, 2):
        xf_z(2, e)
        xf_z(6, e)
    sg_in(3)
    sg_in(5)
    send(sg.at[3 + 2 * c], sg.at[4], ("sg", 4), (z, x, ((y + NY + way) % NY) * 2 + c))
    zf_z(3)
    zf_z(5)
    zf_x(3)
    zf_x(5)
    zf_relay(2)
    zf_relay(6)
    sg_in(4)
    phase("step4")
    for e in (0, 1, 3, 2):
        xf_z(3, e)
        xf_z(5, e)
    zf_z(4)
    zf_x(4)
    for k in range(1, NZ):
        send(nb.at[(z + k) % NZ], nr.at[k], ("nb",), zat(k))
    phase("kproj")
    wait(sg.at[8:16], ("sgm",))
    loads["k"].wait()
    kb[...] = nn(sg[...].reshape(256, 2048), wk[...]).astype(BF16)
    zf_relay(3)
    zf_relay(5)
    phase("vproj")
    loads["v"].wait()
    vb[...] = nn(sg[...].reshape(256, 2048), wv[...]).astype(BF16)
    zf_relay(4)

    def x_sends(k):
        e = 1 if k % 2 == 0 else 3
        send(part.at[k, (x + 2) % NX], reli.at[k], ("rel", k), xat(e))
        send(part.at[k, (x + 4 - e) % NX], xin.at[k, 1], ("xin", k), xat(4 - e))

    def x_relay(k):
        e = 1 if k % 2 == 0 else 3
        wait(reli.at[k], ("rel", k))
        relo[k] = (part[k, (x + e) % NX].astype(F32) + reli[k].astype(F32)).astype(BF16)
        send(relo.at[k], xin.at[k, 0], ("xin", k), xat(e))

    def x_sum(k):
        wait(xin.at[k], ("xin", k))
        return part[k, x].astype(F32) + xin[k, 0].astype(F32) + xin[k, 1].astype(F32)

    def z_send(k):
        if k:
            zout[k] = x_sum(k).astype(BF16)
            send(zout.at[k], zin.at[k], ("zin",), zat(NZ - k))

    def group(k, first):
        q = zf[k, :, 0:64, :].reshape(256, 256)
        h = xf[k].reshape(256, 256)
        stat = jnp.sum(zf[k, :, 64:80, :].astype(F32), axis=0)
        score = nt(kb[...], q)
        prob = jnp.exp(score * SCALE - (SHIFT + stat[0:1]))
        grad = prob * (nt(vb[...], h) - stat[1:2]) * SCALE
        prob = prob.astype(BF16)
        dv_new = nn(prob, h)
        dk_new = nn(grad.astype(BF16), q)
        if first:
            dv[...] = dv_new
            dk[...] = dk_new
        else:
            dv[...] += dv_new
            dk[...] += dk_new
        dq = nn(jnp.transpose(grad).astype(BF16), kb[...])
        part[k] = dq.astype(BF16).reshape(4, 64, 256)

    order = (1, 7, 2, 6, 0, 3, 5, 4)
    for n, k in enumerate(order):
        phase(f"group{n}")
        if k == 3:
            for e in range(4):
                xf_z(4, e)
        zf_end(k)
        group(k, n == 0)
        x_sends(k)
        if n >= 3:
            phase(f"relay{n - 3}")
            x_relay(order[n - 3])
        if n >= 6:
            phase(f"zsend{n - 6}")
            z_send(order[n - 6])

    phase("gmat1")
    dkb = dk[...].astype(BF16)
    dvb = dv[...].astype(BF16)

    def gmat(half):
        lo = 128 * half
        for f in range(4):
            cols = pl.ds(512 * f, 512)
            gout[half, :, :, cols] = (
                (nt(dkb[lo : lo + 128], wk[cols, :]) + nt(dvb[lo : lo + 128], wv[cols, :]))
                .astype(BF16)
                .reshape(8, 16, 512)
            )

    gmat(1)
    send(gout.at[1], gin, ("gm",), mate)
    phase("relay5")
    x_relay(order[5])
    z_send(order[2])
    z_send(order[3])
    phase("relay6")
    x_relay(order[6])
    phase("gmat0")
    gmat(0)
    phase("relay7")
    x_relay(order[7])
    z_send(order[5])
    phase("nrt")
    nr[0] = nb[z]
    wait(nr.at[1:8], ("nb",))
    for j in range(4):
        pair = nr[2 * j : 2 * j + 2].reshape(128, 256).astype(F32)
        nrt[:, 128 * j : 128 * j + 128] = pair.T.astype(BF16)
    phase("zsend")
    z_send(order[6])
    z_send(order[7])
    phase("gsum")
    wait(gin, ("gm",))
    for k in (4, 3, 5, 2, 6, 1, 7):
        gsum[k] = (gout[0, k].astype(F32) + gin[k].astype(F32)).astype(BF16)
        send(gsum.at[k], grecv.at[k], ("g",), yat(NY - k))

    phase("qflat")
    total = x_sum(0)
    wait(zin.at[1:8], ("zin",))
    for k in range(1, NZ):
        total += zin[k].astype(F32)
    qflat = total.astype(BF16)
    qz[0] = qflat
    for k in (4, 3, 5, 2, 6, 1, 7):
        send(qz.at[0], qz.at[k], ("qz",), zat(k))

    phase("ng")
    for f in range(2):
        halves = [nt(qflat, wq[1024 * g + 512 * f : 1024 * g + 512 * f + 512, :]) for g in range(2)]
        for s in range(16):
            nout[s % 2, s // 2, :, 512 * f : 512 * f + 512] = jnp.concatenate(
                [half[4 * s : 4 * s + 4] for half in halves], axis=0
            ).astype(BF16)
    send(nout.at[1 - c], nin, ("nm",), mate)
    phase("nsum")
    wait(nin, ("nm",))
    nsum[...] = (nout[c].astype(F32) + nin[...].astype(F32)).astype(BF16)
    for k in (4, 3, 5, 2, 6, 1, 7):
        send(nsum.at[(y + NY - k) % NY], nrecv.at[k], ("n",), yat(NY - k))

    phase("wmat")
    wait(qz.at[1:8], ("qz",))
    wsum = nn(nrt[...], qz[...].reshape(512, 256))
    wpart[...] = wsum.astype(BF16).reshape(4, 64, 256)
    for e in (2, 1, 3):
        send(wpart.at[(x + e) % NX], win.at[e], ("w",), xat(e))

    phase("gfin")
    wait(grecv.at[1:8], ("g",))
    total = gout[0, 0].astype(F32) + gin[0].astype(F32)
    for k in range(1, NY):
        total += grecv[k].astype(F32)
    sgrad_ref[...] = total

    phase("nfin")
    wait(nrecv.at[1:8], ("n",))
    total = nsum[y].astype(F32)
    for k in range(1, NY):
        total += nrecv[k].astype(F32)
    scaled = jnp.concatenate([total[0:4], total[4:8]], axis=1) * gain
    mean = jnp.mean(scaled * target, axis=1, keepdims=True)
    tgrad_ref[...] = inverse * scaled - target * (inverse * inverse * inverse) * mean

    phase("wfin")
    wait(win.at[1:4], ("w",))
    total = wpart[x].astype(F32)
    for e in range(1, NX):
        total += win[e].astype(F32)
    wgrad_ref[...] = total

    phase("sendwait")
    all_sent = units.at[0 : sent[0]]
    pltpu.make_async_remote_copy(
        src_ref=all_sent, dst_ref=all_sent, send_sem=ssem.at[0], recv_sem=rsem.at[0],
        device_id=mate, device_id_type=MESH,
    ).wait_send()
    phase(None)
    assert sent[0] <= UNITS and len(names) <= RECVS, (sent[0], len(names))


def finish(a_ref, b_ref, c_ref, oa_ref, ob_ref, oc_ref):
    oa_ref[...] = a_ref[...]
    ob_ref[...] = b_ref[...]
    oc_ref[...] = c_ref[...]


def body(tr, sr, gain, wq, wk, wv, wo, saved, offset, og):
    vm = pl.BlockSpec(memory_space=pltpu.VMEM)
    hb = pl.BlockSpec(memory_space=pl.ANY)

    def buf(*shape, dtype=BF16):
        return pltpu.VMEM(shape, dtype)

    outs = (
        jax.ShapeDtypeStruct((4, 2048), F32),
        jax.ShapeDtypeStruct((16, 2048), F32),
        jax.ShapeDtypeStruct((64, 256), F32),
    )
    results = pl.pallas_call(
        kernel,
        out_shape=outs,
        in_specs=[hb] * 10,
        out_specs=(vm, vm, vm),
        scratch_shapes=[
            buf(4, 2048), buf(16, 128), buf(64, 256), buf(1, 64), buf(4, 2048),
            buf(2, 8, 8, 2048), buf(64, 2048, dtype=F32), buf(64, 2048, dtype=F32),
            buf(8, 64, 256), buf(8, 64, 256), buf(256, 512), buf(16, 16, 2048),
            buf(2048, 256), buf(2048, 256), buf(2048, 256), buf(256, 2048),
            buf(8, 4, 80, 256), buf(8, 4, 64, 256),
            buf(256, 256), buf(256, 256),
            buf(256, 256, dtype=F32), buf(256, 256, dtype=F32),
            buf(8, 4, 64, 256), buf(8, 64, 256), buf(8, 64, 256), buf(8, 2, 64, 256),
            buf(8, 64, 256), buf(8, 64, 256),
            buf(8, 64, 256), buf(4, 64, 256), buf(4, 64, 256),
            buf(2, 8, 16, 2048), buf(8, 16, 2048), buf(8, 16, 2048), buf(8, 16, 2048),
            buf(2, 8, 8, 1024), buf(8, 8, 1024), buf(8, 8, 1024), buf(8, 8, 1024),
            buf(UNITS, 16, 256),
            pltpu.SemaphoreType.DMA((1,)),
            pltpu.SemaphoreType.DMA((RECVS,)),
            pltpu.SemaphoreType.DMA((10,)),
        ],
        compiler_params=pltpu.CompilerParams(
            collective_id=0, has_side_effects=True, vmem_limit_bytes=60 * 1024 * 1024
        ),
    )(tr, sr, gain.reshape(16, 128), wq, wk, wv, wo, saved, offset.reshape(1, 64), og)
    return pl.pallas_call(
        finish, out_shape=outs, in_specs=[vm, vm, vm], out_specs=(vm, vm, vm)
    )(*results)


def solution(mesh):
    split = Mesh(mesh.devices.reshape(NZ, NX, mesh.shape["tp"]), ("sp_0", "sp_1", "tp"))
    placed = (
        P(SP_TP, None), P(SP_TP, None), P(), P(None, "tp"), P(None, "tp"), P(None, "tp"),
        P("tp", None), P(SP, "tp"), P(SP, "tp"), P(SP_TP, None),
    )
    return jax.shard_map(
        body,
        mesh=split,
        in_specs=placed,
        out_specs=(P(SP_TP, None), P(SP_TP, None), P(SP, "tp")),
        check_vma=False,
    )
```

```python
import math

import jax
import jax.numpy as jnp
from jax import lax
from jax.experimental import pallas as pl
from jax.experimental.pallas import tpu as pltpu
from jax.sharding import Mesh
from jax.sharding import PartitionSpec as P

SP = ("sp_0", "sp_1")
SP_TP = ("sp_0", "sp_1", "tp")
EPSILON = 1e-06
SCALE = 256 ** (-0.5)
SHIFT = math.log(8192)
MESH = pl.DeviceIdType.MESH
F32 = jnp.float32
BF16 = jnp.bfloat16
NZ, NX, NY = 8, 4, 8
UNIT = 8192
UNITS = 1024
RECVS = 112


def nt(left, right):
    return lax.dot_general(left, right, (((1,), (1,)), ((), ())), preferred_element_type=F32)


def nn(left, right):
    return lax.dot_general(left, right, (((1,), (0,)), ((), ())), preferred_element_type=F32)


def kernel(
    tr_hbm, sr_hbm, gain_hbm, wq_hbm, wk_hbm, wv_hbm, wo_hbm, saved_hbm, off_hbm, og_hbm,
    tgrad_ref, sgrad_ref, wgrad_ref,
    tr, gn, sv, of, og,
    tg, xn, xo, nb, nr, nrt, sg, wq, wk, wv, wo, zf, xf, kb, vb, dk, dv,
    part, near, reli, relo, xin, zout, zin,
    qz, wpart, win,
    gout, gin, gsum, grecv, nout, nin, nsum, nrecv,
    units, ssem, rsem, lsem,
):
    z = lax.axis_index("sp_0")
    x = lax.axis_index("sp_1")
    t = lax.axis_index("tp")
    y = t // 2
    c = t % 2
    way = 1 - 2 * c

    def zat(k):
        return ((z + k) % NZ, x, t)

    def xat(k):
        return (z, (x + k) % NX, t)

    def yat(k):
        return (z, x, ((y + k) % NY) * 2 + c)

    mate = (z, x, t + way)
    names = {}
    sent = [0]
    scope = [None]

    def phase(name):
        if scope[0] is not None:
            scope[0].__exit__(None, None, None)
        scope[0] = jax.named_scope(name) if name else None
        if name:
            scope[0].__enter__()

    def size(ref):
        return math.prod(ref.shape) * 2

    def slot_of(name):
        if name not in names:
            names[name] = len(names)
        return names[name]

    def send(src, dst, name, dev, count=True):
        assert size(src) % UNIT == 0
        sent[0] += count * size(src) // UNIT
        pltpu.make_async_remote_copy(
            src_ref=src, dst_ref=dst, send_sem=ssem.at[0], recv_sem=rsem.at[slot_of(name)],
            device_id=dev, device_id_type=MESH,
        ).start()

    def wait(dst, name):
        pltpu.make_async_remote_copy(
            src_ref=dst, dst_ref=dst, send_sem=ssem.at[0], recv_sem=rsem.at[slot_of(name)],
            device_id=mate, device_id_type=MESH,
        ).wait_recv()

    phase("start")
    loads = {}
    for k, (name, src, dst) in enumerate(
        (
            ("tr", tr_hbm, tr), ("og", og_hbm, og), ("gn", gain_hbm, gn), ("sr", sr_hbm, sg.at[0]),
            ("of", off_hbm, of), ("sv", saved_hbm, sv),
            ("q", wq_hbm, wq), ("o", wo_hbm, wo), ("k", wk_hbm, wk), ("v", wv_hbm, wv),
        )
    ):
        loads[name] = pltpu.make_async_copy(src, dst, lsem.at[k])
        loads[name].start()

    barrier = pltpu.get_barrier_semaphore()
    peers = [mate] + [yat(k) for k in range(1, NY)] + [xat(k) for k in range(1, NX)]
    peers += [zat(k) for k in range(1, NZ)]
    for dev in peers:
        pl.semaphore_signal(barrier, inc=1, device_id=dev, device_id_type=MESH)

    for name in ("tr", "og", "gn"):
        loads[name].wait()
    gain = gn[...].astype(F32)
    gain = jnp.concatenate([gain[s : s + 1] for s in range(16)], axis=1)
    target = tr[...].astype(F32)
    inverse = lax.rsqrt(jnp.mean(target * target, axis=1, keepdims=True) + EPSILON)
    tg[c, y] = jnp.concatenate(
        [target * inverse * gain, og[...].astype(F32)], axis=0
    ).astype(BF16)
    phase("barrier")
    pl.semaphore_wait(barrier, len(peers))

    phase("tgwait")

    def tg_of(k):
        return tg.at[c, (y + NY - k) % NY]

    @pl.when(c == 0)
    def _():
        send(tg_of(0), tg_of(0), ("tg", 4), yat(4), count=False)

    for k in (3, 5, 2, 6, 1, 7):
        send(tg_of(0), tg_of(0), ("tg", k), yat(k))
    send(tg_of(0), tg_of(0), ("tgm",), mate)
    for k in (5, 3, 1, 7, 2, 6, 4):
        wait(tg_of(k), ("tg", k))
        if k == 5:

            @pl.when(c == 1)
            def _():
                send(tg_of(5), tg_of(5), ("tg", 4), yat(7))

        send(tg_of(k), tg_of(k), ("tgm",), mate)
    loads["sr"].wait()
    for k in (2, 6, 1, 7):
        send(sg.at[0], sg.at[k], ("sg", k), yat(k))
    send(sg.at[0], sg.at[8], ("sgm",), mate)
    phase("tgmate")
    wait(tg.at[1 - c], ("tgm",))

    phase("qproj")
    for s in range(16):
        rows = tg[s % 2, s // 2].astype(F32)
        xn[4 * s : 4 * s + 4] = rows[0:4]
        xo[4 * s : 4 * s + 4] = rows[4:8]
    loads["o"].wait()
    hgrad = nt(xo[...].astype(BF16), wo[...]).astype(BF16)
    xf[0, x] = hgrad
    for e in (2, 1, 3):
        send(xf.at[0, x], xf.at[0, x], ("xfx", e), xat(e))
    loads["q"].wait()
    zf[0, x, 0:64] = nn(xn[...].astype(BF16), wq[...]).astype(BF16)
    loads["sv"].wait()
    loads["of"].wait()
    deltas = jnp.sum(hgrad.astype(F32) * sv[...].astype(F32), axis=1, keepdims=True)
    deltas = jnp.broadcast_to(deltas, (64, 128)).T[0:16]
    first = lax.broadcasted_iota(jnp.int32, (16, 64), 0) == 0
    both = jnp.where(first, of[...].astype(F32), deltas).astype(BF16)
    place = lax.broadcasted_iota(jnp.int32, (64, 256), 1) == x * 64 + lax.broadcasted_iota(
        jnp.int32, (64, 256), 0
    )
    zf[0, x, 64:80] = nn(both, place.astype(F32).astype(BF16)).astype(BF16)

    def xs(e):
        return (x + NX - e) % NX

    straight = (3, 5, 4)

    def zf_x(k):
        if k in straight:
            send(zf.at[k, x], zf.at[k, x], ("zfx", k, 2), xat(2))
        send(zf.at[k, x], zf.at[k, x], ("zfx", k, 1), xat(1))
        send(zf.at[k, x], zf.at[k, x], ("zfx", k, 3), xat(3))

    def zf_z(k):
        if k:
            wait(zf.at[k, x], ("zfz", k))
        if k <= 3:
            send(zf.at[k, x], zf.at[k + 1, x], ("zfz", k + 1), zat(1))
        if k == 0 or k >= 6:
            send(zf.at[k, x], zf.at[(k - 1) % NZ, x], ("zfz", (k - 1) % NZ), zat(7))

    def zf_relay(k):
        wait(zf.at[k, xs(1)], ("zfx", k, 1))
        wait(zf.at[k, xs(3)], ("zfx", k, 3))
        if k not in straight:
            e = 1 if k % 2 == 0 else 3
            send(zf.at[k, xs(e)], zf.at[k, xs(e)], ("zfx", k, 2), xat(e))

    def zf_end(k):
        if k in straight:
            zf_relay(k)
        wait(zf.at[k, xs(2)], ("zfx", k, 2))

    def xf_z(k, e):
        if k:
            wait(xf.at[k, xs(e)], ("xfz", k, e))
        if k <= 2 or (k == 3 and e % 2 == 0):
            send(xf.at[k, xs(e)], xf.at[k + 1, xs(e)], ("xfz", k + 1, e), zat(1))
        if k == 0 or k >= 6 or (k == 5 and e % 2 == 1):
            send(xf.at[k, xs(e)], xf.at[(k - 1) % NZ, xs(e)], ("xfz", (k - 1) % NZ, e), zat(7))

    def sg_in(k):
        wait(sg.at[k], ("sg", k))
        if k == 2:
            send(sg.at[2], sg.at[3], ("sg", 3), yat(1))
        if k == 6:
            send(sg.at[6], sg.at[5], ("sg", 5), yat(7))
            send(sg.at[2 + 4 * c], sg.at[4], ("sg", 4), (z, x, ((y + NY + 2 * way) % NY) * 2 + c))
        send(sg.at[k], sg.at[8 + k], ("sgm",), mate)

    phase("spsend")
    zf_z(0)
    xf_z(0, 0)
    zf_x(0)

    phase("step1")
    for f in range(8):
        nb[f] = xn[:, 256 * f : 256 * f + 256].astype(BF16)
    for e in (1, 3):
        wait(xf.at[0, xs(e)], ("xfx", e))
        xf_z(0, e)
    for k in (1, 7):
        zf_z(k)
    wait(xf.at[0, xs(2)], ("xfx", 2))
    xf_z(0, 2)
    for k in (1, 7):
        xf_z(k, 0)
    for k in (1, 7):
        zf_x(k)
    zf_relay(0)
    sg_in(2)
    sg_in(6)
    phase("step2")
    for e in (1, 3):
        xf_z(1, e)
        xf_z(7, e)
    for k in (2, 6):
        zf_z(k)
        xf_z(k, 0)
    for k in (1, 7):
        xf_z(k, 2)
    for k in (2, 6):
        zf_x(k)
    zf_relay(1)
    zf_relay(7)
    sg_in(1)
    sg_in(7)
    phase("step3")
    for e in (1, 3):
        xf_z(2, e)
        xf_z(6, e)
    for k in (3, 5):
        zf_z(k)
        xf_z(k, 0)
    for k in (2, 6):
        xf_z(k, 2)
    for k in (3, 5):
        zf_x(k)
    zf_relay(2)
    zf_relay(6)
    sg_in(3)
    sg_in(5)
    sg_in(4)
    phase("step4")
    for e in (1, 3):
        xf_z(3, e)
        xf_z(5, e)
    zf_z(4)
    zf_x(4)
    for k in (3, 5):
        xf_z(k, 2)
    for k in range(1, NZ):
        send(nb.at[(z + k) % NZ], nr.at[k], ("nb",), zat(k))
    phase("kproj")
    wait(sg.at[8:16], ("sgm",))
    loads["k"].wait()
    kb[...] = nn(sg[...].reshape(256, 2048), wk[...]).astype(BF16)
    phase("vproj")
    loads["v"].wait()
    vb[...] = nn(sg[...].reshape(256, 2048), wv[...]).astype(BF16)

    back = {2: 3, 6: 3, 3: 3, 5: 3}

    def x_sends(k):
        e = back.get(k)
        if e is None:
            for e in (2, 1, 3):
                send(part.at[k, (x + e) % NX], xin.at[k, e - 1], ("xin", k), xat(e))
        else:
            send(part.at[k, (x + 2) % NX], reli.at[k], ("rel", k), xat(e))
            send(part.at[k, (x + 4 - e) % NX], xin.at[k, 1], ("xin", k), xat(4 - e))

    def x_relay(k):
        e = back.get(k)
        if e is None:
            return
        wait(reli.at[k], ("rel", k))
        relo[k] = (part[k, (x + e) % NX].astype(F32) + reli[k].astype(F32)).astype(BF16)
        send(relo.at[k], xin.at[k, 0], ("xin", k), xat(e))

    def x_sum(k):
        count = 2 if k in back else 3
        wait(xin.at[k, 0:count], ("xin", k))
        total = part[k, x].astype(F32)
        for n in range(count):
            total += xin[k, n].astype(F32)
        return total

    def z_send(k):
        if k:
            zout[k] = x_sum(k).astype(BF16)
            send(zout.at[k], zin.at[k], ("zin",), zat(NZ - k))

    def group(k, first):
        q = zf[k, :, 0:64, :].reshape(256, 256)
        h = xf[k].reshape(256, 256)
        stat = jnp.sum(zf[k, :, 64:80, :].astype(F32), axis=0)
        score = nt(kb[...], q)
        prob = jnp.exp(score * SCALE - (SHIFT + stat[0:1]))
        grad = prob * (nt(vb[...], h) - stat[1:2]) * SCALE
        prob = prob.astype(BF16)
        dv_new = nn(prob, h)
        dk_new = nn(grad.astype(BF16), q)
        if first:
            dv[...] = dv_new
            dk[...] = dk_new
        else:
            dv[...] += dv_new
            dk[...] += dk_new
        dq = nn(jnp.transpose(grad).astype(BF16), kb[...])
        part[k] = dq.astype(BF16).reshape(4, 64, 256)

    def work(k, first=False):
        phase(f"group{k}")
        if k == 4:
            for e in range(4):
                xf_z(4, e)
        zf_end(k)
        group(k, first)
        if k in (1, 7):
            send(part.at[k], near.at[k // 7], ("near", k), zat(NZ - k))
        elif k:
            x_sends(k)

    for k in (2, 6, 1, 7, 3):
        work(k, k == 2)
    phase("relay2")
    x_relay(2)
    work(5)
    phase("relay6")
    x_relay(6)
    work(4)
    work(0)
    phase("relay3")
    x_relay(3)
    phase("zsend2")
    z_send(2)

    phase("gmat1")
    dkb = dk[...].astype(BF16)
    dvb = dv[...].astype(BF16)

    def gmat(half):
        lo = 128 * half
        for f in range(4):
            cols = pl.ds(512 * f, 512)
            gout[half, :, :, cols] = (
                (nt(dkb[lo : lo + 128], wk[cols, :]) + nt(dvb[lo : lo + 128], wv[cols, :]))
                .astype(BF16)
                .reshape(8, 16, 512)
            )

    gmat(1)
    send(gout.at[1], gin, ("gm",), mate)
    phase("relay5")
    x_relay(5)
    phase("zsend6")
    z_send(6)
    phase("near")
    wait(near.at[0], ("near", 1))
    wait(near.at[1], ("near", 7))
    part[0] = (part[0].astype(F32) + near[0].astype(F32) + near[1].astype(F32)).astype(BF16)
    x_sends(0)
    phase("gmat0")
    gmat(0)
    phase("zsend3")
    z_send(3)
    phase("zsend5")
    z_send(5)
    phase("zsend4")
    z_send(4)
    phase("gsum")
    wait(gin, ("gm",))
    for k in (4, 3, 5, 2, 6, 1, 7):
        gsum[k] = (gout[0, k].astype(F32) + gin[k].astype(F32)).astype(BF16)
        send(gsum.at[k], grecv.at[k], ("g",), yat(NY - k))

    phase("nrt")
    nr[0] = nb[z]
    wait(nr.at[1:8], ("nb",))
    for j in range(4):
        pair = nr[2 * j : 2 * j + 2].reshape(128, 256).astype(F32)
        nrt[:, 128 * j : 128 * j + 128] = pair.T.astype(BF16)
    phase("qflat")
    total = x_sum(0)
    wait(zin.at[2:7], ("zin",))
    for k in range(2, 7):
        total += zin[k].astype(F32)
    qflat = total.astype(BF16)
    qz[0] = qflat

    @pl.when(c == 0)
    def _():
        send(qz.at[0], qz.at[4], ("qz", 4), zat(4), count=False)

    for k in (3, 5, 2, 6, 1, 7):
        send(qz.at[0], qz.at[k], ("qz", k), zat(k))

    phase("ng")
    for f in range(2):
        halves = [nt(qflat, wq[1024 * g + 512 * f : 1024 * g + 512 * f + 512, :]) for g in range(2)]
        for s in range(16):
            nout[s % 2, s // 2, :, 512 * f : 512 * f + 512] = jnp.concatenate(
                [half[4 * s : 4 * s + 4] for half in halves], axis=0
            ).astype(BF16)
    send(nout.at[1 - c], nin, ("nm",), mate)
    phase("nsum")
    wait(nin, ("nm",))
    nsum[...] = (nout[c].astype(F32) + nin[...].astype(F32)).astype(BF16)
    for k in (4, 3, 5, 2, 6, 1, 7):
        send(nsum.at[(y + NY - k) % NY], nrecv.at[k], ("n",), yat(NY - k))

    phase("wmat")
    wait(qz.at[5], ("qz", 5))

    @pl.when(c == 1)
    def _():
        send(qz.at[5], qz.at[4], ("qz", 4), zat(7))

    for k in (1, 7, 2, 6, 3, 4):
        wait(qz.at[k], ("qz", k))
    wsum = nn(nrt[...], qz[...].reshape(512, 256))
    wpart[...] = wsum.astype(BF16).reshape(4, 64, 256)
    for e in (2, 1, 3):
        send(wpart.at[(x + e) % NX], win.at[e], ("w",), xat(e))

    phase("gfin")
    wait(grecv.at[1:8], ("g",))
    total = gout[0, 0].astype(F32) + gin[0].astype(F32)
    for k in range(1, NY):
        total += grecv[k].astype(F32)
    sgrad_ref[...] = total

    phase("nfin")
    wait(nrecv.at[1:8], ("n",))
    total = nsum[y].astype(F32)
    for k in range(1, NY):
        total += nrecv[k].astype(F32)
    scaled = jnp.concatenate([total[0:4], total[4:8]], axis=1) * gain
    mean = jnp.mean(scaled * target, axis=1, keepdims=True)
    tgrad_ref[...] = inverse * scaled - target * (inverse * inverse * inverse) * mean

    phase("wfin")
    wait(win.at[1:4], ("w",))
    total = wpart[x].astype(F32)
    for e in range(1, NX):
        total += win[e].astype(F32)
    wgrad_ref[...] = total

    phase("sendwait")
    all_sent = units.at[0 : sent[0]]
    pltpu.make_async_remote_copy(
        src_ref=all_sent, dst_ref=all_sent, send_sem=ssem.at[0], recv_sem=rsem.at[0],
        device_id=mate, device_id_type=MESH,
    ).wait_send()
    phase(None)
    assert sent[0] <= UNITS and len(names) <= RECVS, (sent[0], len(names))


def finish(a_ref, b_ref, c_ref, oa_ref, ob_ref, oc_ref):
    oa_ref[...] = a_ref[...]
    ob_ref[...] = b_ref[...]
    oc_ref[...] = c_ref[...]


def body(tr, sr, gain, wq, wk, wv, wo, saved, offset, og):
    vm = pl.BlockSpec(memory_space=pltpu.VMEM)
    hb = pl.BlockSpec(memory_space=pl.ANY)

    def buf(*shape, dtype=BF16):
        return pltpu.VMEM(shape, dtype)

    outs = (
        jax.ShapeDtypeStruct((4, 2048), F32),
        jax.ShapeDtypeStruct((16, 2048), F32),
        jax.ShapeDtypeStruct((64, 256), F32),
    )
    results = pl.pallas_call(
        kernel,
        out_shape=tuple(pltpu.VMEM(o.shape, o.dtype) for o in outs),
        in_specs=[hb] * 10,
        out_specs=(vm, vm, vm),
        scratch_shapes=[
            buf(4, 2048), buf(16, 128), buf(64, 256), buf(1, 64), buf(4, 2048),
            buf(2, 8, 8, 2048), buf(64, 2048, dtype=F32), buf(64, 2048, dtype=F32),
            buf(8, 64, 256), buf(8, 64, 256), buf(256, 512), buf(16, 16, 2048),
            buf(2048, 256), buf(2048, 256), buf(2048, 256), buf(256, 2048),
            buf(8, 4, 80, 256), buf(8, 4, 64, 256),
            buf(256, 256), buf(256, 256),
            buf(256, 256, dtype=F32), buf(256, 256, dtype=F32),
            buf(8, 4, 64, 256), buf(2, 4, 64, 256), buf(8, 64, 256), buf(8, 64, 256),
            buf(8, 3, 64, 256),
            buf(8, 64, 256), buf(8, 64, 256),
            buf(8, 64, 256), buf(4, 64, 256), buf(4, 64, 256),
            buf(2, 8, 16, 2048), buf(8, 16, 2048), buf(8, 16, 2048), buf(8, 16, 2048),
            buf(2, 8, 8, 1024), buf(8, 8, 1024), buf(8, 8, 1024), buf(8, 8, 1024),
            buf(UNITS, 16, 256),
            pltpu.SemaphoreType.DMA((1,)),
            pltpu.SemaphoreType.DMA((RECVS,)),
            pltpu.SemaphoreType.DMA((10,)),
        ],
        compiler_params=pltpu.CompilerParams(
            collective_id=0, has_side_effects=True, vmem_limit_bytes=60 * 1024 * 1024
        ),
    )(tr, sr, gain.reshape(16, 128), wq, wk, wv, wo, saved, offset.reshape(1, 64), og)
    return pl.pallas_call(
        finish, out_shape=outs, in_specs=[vm, vm, vm], out_specs=(vm, vm, vm)
    )(*[pltpu.with_memory_space_constraint(r, pltpu.VMEM) for r in results])


def solution(mesh):
    split = Mesh(mesh.devices.reshape(NZ, NX, mesh.shape["tp"]), ("sp_0", "sp_1", "tp"))
    placed = (
        P(SP_TP, None), P(SP_TP, None), P(), P(None, "tp"), P(None, "tp"), P(None, "tp"),
        P("tp", None), P(SP, "tp"), P(SP, "tp"), P(SP_TP, None),
    )
    return jax.shard_map(
        body,
        mesh=split,
        in_specs=placed,
        out_specs=(P(SP_TP, None), P(SP_TP, None), P(SP, "tp")),
        check_vma=False,
    )
```

```python
import math

import jax
import jax.numpy as jnp
from jax import lax
from jax.experimental import pallas as pl
from jax.experimental.pallas import tpu as pltpu
from jax.sharding import Mesh
from jax.sharding import PartitionSpec as P

SP = ("sp_0", "sp_1")
SP_TP = ("sp_0", "sp_1", "tp")
EPSILON = 1e-06
SCALE = 256 ** (-0.5)
SHIFT = math.log(8192)
MESH = pl.DeviceIdType.MESH
F32 = jnp.float32
BF16 = jnp.bfloat16
NZ, NX, NY = 8, 4, 8
UNIT = 2048
UNITS = 4096
RECVS = 112


def nt(left, right):
    return lax.dot_general(left, right, (((1,), (1,)), ((), ())), preferred_element_type=F32)


def nn(left, right):
    return lax.dot_general(left, right, (((1,), (0,)), ((), ())), preferred_element_type=F32)


def kernel(
    tr_hbm, sr_hbm, gain_hbm, wq_hbm, wk_hbm, wv_hbm, wo_hbm, saved_hbm, off_hbm, og_hbm,
    tgrad_ref, sgrad_ref, wgrad_ref,
    tr, gn, sv, of, og,
    tg, xn, xo, nzs, nza, nyb, nr, nrt, sg, wq, wk, wv, wo, zf, xf, kb, vb, dk, dv,
    part, near, xin, zout, zin,
    qz, wpart, win,
    gout, gin, gsum, gmid, grecv, nout, nin, nsum, nrecv,
    units, ssem, rsem, lsem,
):
    z = lax.axis_index("sp_0")
    x = lax.axis_index("sp_1")
    t = lax.axis_index("tp")
    y = t // 2
    c = t % 2
    way = 1 - 2 * c

    def zat(k):
        return ((z + k) % NZ, x, t)

    def xat(k):
        return (z, (x + k) % NX, t)

    def yat(k):
        return (z, x, ((y + k) % NY) * 2 + c)

    mate = (z, x, t + way)
    names = {}
    sent = [0]
    scope = [None]

    def phase(name):
        if scope[0] is not None:
            scope[0].__exit__(None, None, None)
        scope[0] = jax.named_scope(name) if name else None
        if name:
            scope[0].__enter__()

    def size(ref):
        return math.prod(ref.shape) * 2

    def slot_of(name):
        if name not in names:
            names[name] = len(names)
        return names[name]

    def send(src, dst, name, dev, count=True):
        assert size(src) % UNIT == 0
        sent[0] += count * size(src) // UNIT
        pltpu.make_async_remote_copy(
            src_ref=src, dst_ref=dst, send_sem=ssem.at[0], recv_sem=rsem.at[slot_of(name)],
            device_id=dev, device_id_type=MESH,
        ).start()

    def wait(dst, name):
        pltpu.make_async_remote_copy(
            src_ref=dst, dst_ref=dst, send_sem=ssem.at[0], recv_sem=rsem.at[slot_of(name)],
            device_id=mate, device_id_type=MESH,
        ).wait_recv()

    phase("start")
    loads = {}
    for k, (name, src, dst) in enumerate(
        (
            ("tr", tr_hbm, tr), ("og", og_hbm, og), ("gn", gain_hbm, gn), ("sr", sr_hbm, sg.at[0]),
            ("of", off_hbm, of), ("sv", saved_hbm, sv),
            ("q", wq_hbm, wq), ("o", wo_hbm, wo), ("k", wk_hbm, wk), ("v", wv_hbm, wv),
        )
    ):
        loads[name] = pltpu.make_async_copy(src, dst, lsem.at[k])
        loads[name].start()

    barrier = pltpu.get_barrier_semaphore()
    peers = [mate] + [yat(k) for k in range(1, NY)] + [xat(k) for k in range(1, NX)]
    peers += [zat(k) for k in range(1, NZ)]
    for dev in peers:
        pl.semaphore_signal(barrier, inc=1, device_id=dev, device_id_type=MESH)

    for name in ("tr", "og", "gn"):
        loads[name].wait()
    gain = gn[...].astype(F32)
    gain = jnp.concatenate([gain[s : s + 1] for s in range(16)], axis=1)
    target = tr[...].astype(F32)
    inverse = lax.rsqrt(jnp.mean(target * target, axis=1, keepdims=True) + EPSILON)
    normed = target * inverse * gain
    tg[c, y] = jnp.concatenate([normed, og[...].astype(F32)], axis=0).astype(BF16)
    for f in range(NZ):
        nzs[f] = normed[:, 256 * f : 256 * f + 256].astype(BF16)
    phase("barrier")
    pl.semaphore_wait(barrier, len(peers))

    phase("tgwait")

    def tg_of(k):
        return tg.at[c, (y + NY - k) % NY]

    for k in (4, 3, 5, 2, 6, 1, 7):
        send(tg_of(0), tg_of(0), ("tg", k), yat(k))
    send(tg_of(0), tg_of(0), ("tgm",), mate)
    for k in range(1, NZ):
        send(nzs.at[(z + k) % NZ], nza.at[k], ("nza",), zat(k))
    for k in (1, 7, 2, 6, 3, 5, 4):
        wait(tg_of(k), ("tg", k))
        send(tg_of(k), tg_of(k), ("tgm",), mate)
    loads["sr"].wait()
    for k in (2, 6, 1, 7):
        send(sg.at[0], sg.at[k], ("sg", k), yat(k))
    send(sg.at[0], sg.at[8], ("sgm",), mate)
    phase("tgmate")
    wait(tg.at[1 - c], ("tgm",))

    phase("qproj")
    for s in range(16):
        rows = tg[s % 2, s // 2].astype(F32)
        xn[4 * s : 4 * s + 4] = rows[0:4]
        xo[4 * s : 4 * s + 4] = rows[4:8]
    loads["o"].wait()
    hgrad = nt(xo[...].astype(BF16), wo[...]).astype(BF16)
    xf[0, x] = hgrad
    for e in (2, 1, 3):
        send(xf.at[0, x], xf.at[0, x], ("xfx", e), xat(e))
    loads["q"].wait()
    zf[0, x, 0:64] = nn(xn[...].astype(BF16), wq[...]).astype(BF16)
    loads["sv"].wait()
    loads["of"].wait()
    deltas = jnp.sum(hgrad.astype(F32) * sv[...].astype(F32), axis=1, keepdims=True)
    deltas = jnp.broadcast_to(deltas, (64, 128)).T[0:16]
    first = lax.broadcasted_iota(jnp.int32, (16, 64), 0) == 0
    both = jnp.where(first, of[...].astype(F32), deltas).astype(BF16)
    place = lax.broadcasted_iota(jnp.int32, (64, 256), 1) == x * 64 + lax.broadcasted_iota(
        jnp.int32, (64, 256), 0
    )
    zf[0, x, 64:80] = nn(both, place.astype(F32).astype(BF16)).astype(BF16)

    def xs(e):
        return (x + NX - e) % NX

    def zf_x(k):
        for e in (2, 1, 3):
            send(zf.at[k, x], zf.at[k, x], ("zfx", k, e), xat(e))

    def zf_z(k):
        if k:
            wait(zf.at[k, x], ("zfz", k))
        if k <= 3:
            send(zf.at[k, x], zf.at[k + 1, x], ("zfz", k + 1), zat(1))
        if k == 0 or k >= 6:
            send(zf.at[k, x], zf.at[(k - 1) % NZ, x], ("zfz", (k - 1) % NZ), zat(7))

    def zf_end(k):
        for e in (1, 3, 2):
            wait(zf.at[k, xs(e)], ("zfx", k, e))

    def xf_z(k, e):
        if k:
            wait(xf.at[k, xs(e)], ("xfz", k, e))
        if k <= 2 or (k == 3 and e % 2 == 0):
            send(xf.at[k, xs(e)], xf.at[k + 1, xs(e)], ("xfz", k + 1, e), zat(1))
        if k == 0 or k >= 6 or (k == 5 and e % 2 == 1):
            send(xf.at[k, xs(e)], xf.at[(k - 1) % NZ, xs(e)], ("xfz", (k - 1) % NZ, e), zat(7))

    def sg_in(k):
        wait(sg.at[k], ("sg", k))
        if k == 2:
            send(sg.at[2], sg.at[3], ("sg", 3), yat(1))
        if k == 6:
            send(sg.at[6], sg.at[5], ("sg", 5), yat(7))
            send(sg.at[2 + 4 * c], sg.at[4], ("sg", 4), (z, x, ((y + NY + 2 * way) % NY) * 2 + c))
        send(sg.at[k], sg.at[8 + k], ("sgm",), mate)

    def x_sends(k):
        for e in (2, 1, 3):
            send(part.at[k, (x + e) % NX], xin.at[k, e - 1], ("xin", k), xat(e))

    def x_sum(k):
        wait(xin.at[k], ("xin", k))
        total = part[k, x].astype(F32)
        for n in range(3):
            total += xin[k, n].astype(F32)
        return total

    def z_send(k):
        if k:
            zout[k] = x_sum(k).astype(BF16)
            send(zout.at[k], zin.at[k], ("zin",), zat(NZ - k))

    def group(k, first):
        q = zf[k, :, 0:64, :].reshape(256, 256)
        h = xf[k].reshape(256, 256)
        stat = jnp.sum(zf[k, :, 64:80, :].astype(F32), axis=0)
        score = nt(kb[...], q)
        prob = jnp.exp(score * SCALE - (SHIFT + stat[0:1]))
        grad = prob * (nt(vb[...], h) - stat[1:2]) * SCALE
        prob = prob.astype(BF16)
        dv_new = nn(prob, h)
        dk_new = nn(grad.astype(BF16), q)
        if first:
            dv[...] = dv_new
            dk[...] = dk_new
        else:
            dv[...] += dv_new
            dk[...] += dk_new
        dq = nn(jnp.transpose(grad).astype(BF16), kb[...])
        part[k] = dq.astype(BF16).reshape(4, 64, 256)

    def work(k, first=False):
        phase(f"group{k}")
        zf_end(k)
        group(k, first)
        if k not in (0, 1, 7):
            x_sends(k)

    phase("spsend")
    zf_z(0)
    xf_z(0, 0)
    zf_x(0)

    phase("step1")
    for e in (1, 3):
        wait(xf.at[0, xs(e)], ("xfx", e))
        xf_z(0, e)
    for k in (1, 7):
        zf_z(k)
    wait(xf.at[0, xs(2)], ("xfx", 2))
    xf_z(0, 2)
    for k in (1, 7):
        xf_z(k, 0)
    for k in (1, 7):
        zf_x(k)
    sg_in(2)
    sg_in(6)
    phase("step2")
    for e in (1, 3):
        xf_z(1, e)
        xf_z(7, e)
    for k in (2, 6):
        zf_z(k)
        xf_z(k, 0)
    for k in (1, 7):
        xf_z(k, 2)
    for k in (2, 6):
        zf_x(k)
    for k in (1, 7, 3, 5, 4):
        sg_in(k)
    nza[0] = nzs[z]
    wait(nza.at[1:8], ("nza",))
    nyb[c, y] = nza[...]
    for k in (4, 3, 5, 2, 6, 1, 7):
        send(nza, nyb.at[c, y], ("nyb",), yat(k))
    send(nza, nyb.at[c, y], ("nybm",), mate)
    phase("step3")
    for e in (1, 3):
        xf_z(2, e)
        xf_z(6, e)
    for k in (3, 5):
        zf_z(k)
        xf_z(k, 0)
    for k in (2, 6):
        xf_z(k, 2)
    for k in (3, 5):
        zf_x(k)
    phase("kproj")
    wait(sg.at[8:16], ("sgm",))
    loads["k"].wait()
    kb[...] = nn(sg[...].reshape(256, 2048), wk[...]).astype(BF16)
    phase("vproj")
    loads["v"].wait()
    vb[...] = nn(sg[...].reshape(256, 2048), wv[...]).astype(BF16)
    work(1, True)
    work(7)
    phase("step4")
    for e in (1, 3):
        xf_z(3, e)
        xf_z(5, e)
    zf_z(4)
    zf_x(4)
    for k in (3, 5):
        xf_z(k, 2)
    for k in (1, 7):
        send(part.at[k], near.at[k // 7], ("near", k), zat(NZ - k))
    phase("nyb")
    wait(nyb.at[0, 0:7], ("nyb",))
    for k in range(1, NY):
        send(nyb.at[c, (y + k) % NY], nyb.at[c, (y + k) % NY], ("nybm",), mate)
    work(2)
    work(6)
    work(0)
    phase("xf4")
    for e in range(4):
        xf_z(4, e)
    work(3)
    work(5)
    work(4)

    phase("gmat1")
    dkb = dk[...].astype(BF16)
    dvb = dv[...].astype(BF16)

    def gmat(half):
        lo = 128 * half
        for f in range(4):
            cols = pl.ds(512 * f, 512)
            gout[half, :, :, cols] = (
                (nt(dkb[lo : lo + 128], wk[cols, :]) + nt(dvb[lo : lo + 128], wv[cols, :]))
                .astype(BF16)
                .reshape(8, 16, 512)
            )

    gmat(1)
    send(gout.at[1], gin, ("gm",), mate)
    phase("zsend2")
    z_send(2)
    phase("gmat0")
    gmat(0)
    phase("zsend6")
    z_send(6)
    phase("near")
    wait(near.at[0], ("near", 1))
    wait(near.at[1], ("near", 7))
    part[0] = (part[0].astype(F32) + near[0].astype(F32) + near[1].astype(F32)).astype(BF16)
    x_sends(0)
    phase("zsend3")
    z_send(3)
    phase("zsend5")
    z_send(5)
    phase("zsend4")
    z_send(4)
    phase("nrt")
    wait(nyb.at[0], ("nybm",))
    for s in range(16):
        rows = nyb[s % 2, s // 2].astype(F32)
        for k in range(NZ):
            nr[k, 4 * s : 4 * s + 4] = rows[k]
    for j in range(4):
        pair = nr[2 * j : 2 * j + 2].reshape(128, 256)
        nrt[:, 128 * j : 128 * j + 128] = pair.T.astype(BF16)
    phase("gsum")
    wait(gin, ("gm",))
    for k in (4, 3, 5, 1, 7):
        gsum[k] = (gout[0, k].astype(F32) + gin[k].astype(F32)).astype(BF16)
    send(gsum.at[4], gmid.at[2], ("gmid",), yat((NY - 2 * way) % NY))
    send(gsum.at[3], gmid.at[0], ("gmid",), yat(7))
    send(gsum.at[5], gmid.at[1], ("gmid",), yat(1))
    send(gsum.at[1], grecv.at[1], ("g",), yat(7))
    send(gsum.at[7], grecv.at[7], ("g",), yat(1))
    phase("qflat")
    total = x_sum(0)
    wait(zin.at[2:7], ("zin",))
    for k in range(2, 7):
        total += zin[k].astype(F32)
    qflat = total.astype(BF16)
    qz[0] = qflat

    for k in (4, 3, 5, 2, 6, 1, 7):
        send(qz.at[0], qz.at[k], ("qz",), zat(k))

    phase("ng")
    for f in range(2):
        halves = [nt(qflat, wq[1024 * g + 512 * f : 1024 * g + 512 * f + 512, :]) for g in range(2)]
        for s in range(16):
            nout[s % 2, s // 2, :, 512 * f : 512 * f + 512] = jnp.concatenate(
                [half[4 * s : 4 * s + 4] for half in halves], axis=0
            ).astype(BF16)
    send(nout.at[1 - c], nin, ("nm",), mate)
    phase("gmid")
    wait(gmid, ("gmid",))
    for k, n in ((2, 0), (6, 1)):
        mid = jnp.where(c == n, gmid[2].astype(F32), 0.0) + gmid[n].astype(F32)
        gsum[k] = (gout[0, k].astype(F32) + gin[k].astype(F32) + mid).astype(BF16)
        send(gsum.at[k], grecv.at[k], ("g",), yat(NY - k))
    phase("nsum")
    wait(nin, ("nm",))
    nsum[...] = (nout[c].astype(F32) + nin[...].astype(F32)).astype(BF16)
    for k in (4, 3, 5, 2, 6, 1, 7):
        send(nsum.at[(y + NY - k) % NY], nrecv.at[k], ("n",), yat(NY - k))

    phase("wmat")
    wait(qz.at[1:8], ("qz",))
    wsum = nn(nrt[...], qz[...].reshape(512, 256))
    wpart[...] = wsum.astype(BF16).reshape(4, 64, 256)
    for e in (2, 1, 3):
        send(wpart.at[(x + e) % NX], win.at[e], ("w",), xat(e))

    phase("gfin")
    wait(grecv.at[0:4], ("g",))
    total = gout[0, 0].astype(F32) + gin[0].astype(F32)
    for k in (1, 2, 6, 7):
        total += grecv[k].astype(F32)
    sgrad_ref[...] = total

    phase("nfin")
    wait(nrecv.at[1:8], ("n",))
    total = nsum[y].astype(F32)
    for k in range(1, NY):
        total += nrecv[k].astype(F32)
    scaled = jnp.concatenate([total[0:4], total[4:8]], axis=1) * gain
    mean = jnp.mean(scaled * target, axis=1, keepdims=True)
    tgrad_ref[...] = inverse * scaled - target * (inverse * inverse * inverse) * mean

    phase("wfin")
    wait(win.at[1:4], ("w",))
    total = wpart[x].astype(F32)
    for e in range(1, NX):
        total += win[e].astype(F32)
    wgrad_ref[...] = total

    phase("sendwait")
    all_sent = units.at[0 : sent[0]]
    pltpu.make_async_remote_copy(
        src_ref=all_sent, dst_ref=all_sent, send_sem=ssem.at[0], recv_sem=rsem.at[0],
        device_id=mate, device_id_type=MESH,
    ).wait_send()
    phase(None)
    assert sent[0] <= UNITS and len(names) <= RECVS, (sent[0], len(names))


def finish(a_ref, b_ref, c_ref, oa_ref, ob_ref, oc_ref):
    oa_ref[...] = a_ref[...]
    ob_ref[...] = b_ref[...]
    oc_ref[...] = c_ref[...]


def body(tr, sr, gain, wq, wk, wv, wo, saved, offset, og):
    vm = pl.BlockSpec(memory_space=pltpu.VMEM)
    hb = pl.BlockSpec(memory_space=pl.ANY)

    def buf(*shape, dtype=BF16):
        return pltpu.VMEM(shape, dtype)

    outs = (
        jax.ShapeDtypeStruct((4, 2048), F32),
        jax.ShapeDtypeStruct((16, 2048), F32),
        jax.ShapeDtypeStruct((64, 256), F32),
    )
    results = pl.pallas_call(
        kernel,
        out_shape=tuple(pltpu.VMEM(o.shape, o.dtype) for o in outs),
        in_specs=[hb] * 10,
        out_specs=(vm, vm, vm),
        scratch_shapes=[
            buf(4, 2048), buf(16, 128), buf(64, 256), buf(1, 64), buf(4, 2048),
            buf(2, 8, 8, 2048), buf(64, 2048, dtype=F32), buf(64, 2048, dtype=F32),
            buf(8, 4, 256), buf(8, 4, 256), buf(2, 8, 8, 4, 256),
            buf(8, 64, 256, dtype=F32), buf(256, 512), buf(16, 16, 2048),
            buf(2048, 256), buf(2048, 256), buf(2048, 256), buf(256, 2048),
            buf(8, 4, 80, 256), buf(8, 4, 64, 256),
            buf(256, 256), buf(256, 256),
            buf(256, 256, dtype=F32), buf(256, 256, dtype=F32),
            buf(8, 4, 64, 256), buf(2, 4, 64, 256),
            buf(8, 3, 64, 256),
            buf(8, 64, 256), buf(8, 64, 256),
            buf(8, 64, 256), buf(4, 64, 256), buf(4, 64, 256),
            buf(2, 8, 16, 2048), buf(8, 16, 2048), buf(8, 16, 2048), buf(3, 16, 2048), buf(8, 16, 2048),
            buf(2, 8, 8, 1024), buf(8, 8, 1024), buf(8, 8, 1024), buf(8, 8, 1024),
            buf(UNITS, 4, 256),
            pltpu.SemaphoreType.DMA((1,)),
            pltpu.SemaphoreType.DMA((RECVS,)),
            pltpu.SemaphoreType.DMA((10,)),
        ],
        compiler_params=pltpu.CompilerParams(
            collective_id=0, has_side_effects=True, vmem_limit_bytes=60 * 1024 * 1024
        ),
    )(tr, sr, gain.reshape(16, 128), wq, wk, wv, wo, saved, offset.reshape(1, 64), og)
    return pl.pallas_call(
        finish, out_shape=outs, in_specs=[vm, vm, vm], out_specs=(vm, vm, vm)
    )(*[pltpu.with_memory_space_constraint(r, pltpu.VMEM) for r in results])


def solution(mesh):
    split = Mesh(mesh.devices.reshape(NZ, NX, mesh.shape["tp"]), ("sp_0", "sp_1", "tp"))
    placed = (
        P(SP_TP, None), P(SP_TP, None), P(), P(None, "tp"), P(None, "tp"), P(None, "tp"),
        P("tp", None), P(SP, "tp"), P(SP, "tp"), P(SP_TP, None),
    )
    return jax.shard_map(
        body,
        mesh=split,
        in_specs=placed,
        out_specs=(P(SP_TP, None), P(SP_TP, None), P(SP, "tp")),
        check_vma=False,
    )
```

```python
import math

import jax
import jax.numpy as jnp
from jax import lax
from jax.experimental import pallas as pl
from jax.experimental.pallas import tpu as pltpu
from jax.sharding import Mesh
from jax.sharding import PartitionSpec as P

SP = ("sp_0", "sp_1")
SP_TP = ("sp_0", "sp_1", "tp")
EPSILON = 1e-06
SCALE = 256 ** (-0.5)
SHIFT = math.log(8192)
MESH = pl.DeviceIdType.MESH
F32 = jnp.float32
BF16 = jnp.bfloat16
NZ, NX, NY = 8, 4, 8
UNIT = 2048
UNITS = 4096
RECVS = 112


def nt(left, right):
    return lax.dot_general(left, right, (((1,), (1,)), ((), ())), preferred_element_type=F32)


def nn(left, right):
    return lax.dot_general(left, right, (((1,), (0,)), ((), ())), preferred_element_type=F32)


def kernel(
    tr_hbm, sr_hbm, gain_hbm, wq_hbm, wk_hbm, wv_hbm, wo_hbm, saved_hbm, off_hbm, og_hbm,
    tgrad_ref, sgrad_ref, wgrad_ref,
    tr, gn, sv, of, og,
    tg, xn, xo, nzs, nza, nyb, nr, nrt, sg, wq, wk, wv, wo, zf, xf, kb, vb, dk, dv,
    part, near, xin, zout, zin,
    qz, wpart, win,
    gout, gin, gsum, gmid, grecv, nout, nin, nsum, nrecv,
    units, ssem, rsem, lsem,
):
    z = lax.axis_index("sp_0")
    x = lax.axis_index("sp_1")
    t = lax.axis_index("tp")
    y = t // 2
    c = t % 2
    way = 1 - 2 * c

    def zat(k):
        return ((z + k) % NZ, x, t)

    def xat(k):
        return (z, (x + k) % NX, t)

    def yat(k):
        return (z, x, ((y + k) % NY) * 2 + c)

    mate = (z, x, t + way)
    names = {}
    sent = [0, 0]
    scope = [None]

    def phase(name):
        if scope[0] is not None:
            scope[0].__exit__(None, None, None)
        scope[0] = jax.named_scope(name) if name else None
        if name:
            scope[0].__enter__()

    def size(ref):
        return math.prod(ref.shape) * 2

    def slot_of(name):
        if name not in names:
            names[name] = len(names)
        return names[name]

    def send(src, dst, name, dev, sem=0):
        assert size(src) % UNIT == 0
        sent[sem] += size(src) // UNIT
        pltpu.make_async_remote_copy(
            src_ref=src, dst_ref=dst, send_sem=ssem.at[sem], recv_sem=rsem.at[slot_of(name)],
            device_id=dev, device_id_type=MESH,
        ).start()

    def wait(dst, name):
        pltpu.make_async_remote_copy(
            src_ref=dst, dst_ref=dst, send_sem=ssem.at[0], recv_sem=rsem.at[slot_of(name)],
            device_id=mate, device_id_type=MESH,
        ).wait_recv()

    phase("start")
    loads = {}
    for k, (name, src, dst) in enumerate(
        (
            ("tr", tr_hbm, tr), ("og", og_hbm, og), ("gn", gain_hbm, gn), ("sr", sr_hbm, sg.at[c, 0]),
            ("of", off_hbm, of), ("sv", saved_hbm, sv),
            ("q", wq_hbm, wq), ("o", wo_hbm, wo), ("k", wk_hbm, wk), ("v", wv_hbm, wv),
        )
    ):
        loads[name] = pltpu.make_async_copy(src, dst, lsem.at[k])
        loads[name].start()

    barrier = pltpu.get_barrier_semaphore()
    peers = [mate] + [yat(k) for k in range(1, NY)] + [xat(k) for k in range(1, NX)]
    peers += [zat(k) for k in range(1, NZ)]
    for dev in peers:
        pl.semaphore_signal(barrier, inc=1, device_id=dev, device_id_type=MESH)

    for name in ("tr", "og", "gn"):
        loads[name].wait()
    gain = gn[...].astype(F32)
    gain = jnp.concatenate([gain[s : s + 1] for s in range(16)], axis=1)
    target = tr[...].astype(F32)
    inverse = lax.rsqrt(jnp.mean(target * target, axis=1, keepdims=True) + EPSILON)
    normed = target * inverse * gain
    tg[c, y] = jnp.concatenate([normed, og[...].astype(F32)], axis=0).astype(BF16)
    for f in range(NZ):
        nzs[f] = normed[:, 256 * f : 256 * f + 256].astype(BF16)
    phase("barrier")
    pl.semaphore_wait(barrier, len(peers))

    phase("tgwait")
    loads["sr"].wait()
    send(sg.at[c, 0], sg.at[c, 0], ("sg0",), mate)

    def tg_of(k):
        return tg.at[c, (y + NY - k) % NY]

    for k in (4, 3, 5, 2, 6, 1, 7):
        send(tg_of(0), tg_of(0), ("tg", k), yat(k))
    send(tg_of(0), tg_of(0), ("tgm",), mate)
    for k in range(1, NZ):
        send(nzs.at[(z + k) % NZ], nza.at[k], ("nza",), zat(k))
    for k in (1, 7, 2, 6, 3, 5, 4):
        wait(tg_of(k), ("tg", k))
        send(tg_of(k), tg_of(k), ("tgm",), mate)

    @pl.when(c == 1)
    def _():
        wait(sg.at[0, 0], ("sg0",))
        for k in (2, 6, 1, 7):
            send(sg.at[:, 0], sg.at[:, k], ("sg", k), yat(k), 1)

    phase("tgmate")
    wait(tg.at[1 - c], ("tgm",))

    phase("qproj")
    for s in range(16):
        rows = tg[s % 2, s // 2].astype(F32)
        xn[4 * s : 4 * s + 4] = rows[0:4]
        xo[4 * s : 4 * s + 4] = rows[4:8]
    loads["o"].wait()
    hgrad = nt(xo[...].astype(BF16), wo[...]).astype(BF16)
    xf[0, x] = hgrad
    for e in (2, 1, 3):
        send(xf.at[0, x], xf.at[0, x], ("xfx", e), xat(e))
    loads["q"].wait()
    zf[0, x, 0:64] = nn(xn[...].astype(BF16), wq[...]).astype(BF16)
    loads["sv"].wait()
    loads["of"].wait()
    deltas = jnp.sum(hgrad.astype(F32) * sv[...].astype(F32), axis=1, keepdims=True)
    deltas = jnp.broadcast_to(deltas, (64, 128)).T[0:16]
    first = lax.broadcasted_iota(jnp.int32, (16, 64), 0) == 0
    both = jnp.where(first, of[...].astype(F32), deltas).astype(BF16)
    place = lax.broadcasted_iota(jnp.int32, (64, 256), 1) == x * 64 + lax.broadcasted_iota(
        jnp.int32, (64, 256), 0
    )
    zf[0, x, 64:72] = nn(both, place.astype(F32).astype(BF16))[0:8].astype(BF16)

    def xs(e):
        return (x + NX - e) % NX

    def zf_x(k):
        for e in (2, 1, 3):
            send(zf.at[k, x], zf.at[k, x], ("zfx", k, e), xat(e))

    def zf_z(k):
        if k:
            wait(zf.at[k, x], ("zfz", k))
        if k <= 3:
            send(zf.at[k, x], zf.at[k + 1, x], ("zfz", k + 1), zat(1))
        if k == 0 or k >= 6:
            send(zf.at[k, x], zf.at[(k - 1) % NZ, x], ("zfz", (k - 1) % NZ), zat(7))

    def zf_end(k):
        for e in (1, 3, 2):
            wait(zf.at[k, xs(e)], ("zfx", k, e))

    def xf_z(k, e):
        if k:
            wait(xf.at[k, xs(e)], ("xfz", k, e))
        if k <= 2 or (k == 3 and e % 2 == 0):
            send(xf.at[k, xs(e)], xf.at[k + 1, xs(e)], ("xfz", k + 1, e), zat(1))
        if k == 0 or k >= 6 or (k == 5 and e % 2 == 1):
            send(xf.at[k, xs(e)], xf.at[(k - 1) % NZ, xs(e)], ("xfz", (k - 1) % NZ, e), zat(7))

    def sg_in(*ks):
        @pl.when(c == 1)
        def _():
            for k in ks:
                wait(sg.at[:, k], ("sg", k))
                if k == 2:
                    send(sg.at[:, 2], sg.at[:, 3], ("sg", 3), yat(1), 1)
                    send(sg.at[0, 2], sg.at[0, 4], ("sg", 4), yat(2), 1)
                if k == 6:
                    send(sg.at[:, 6], sg.at[:, 5], ("sg", 5), yat(7), 1)
                    send(sg.at[1, 6], sg.at[1, 4], ("sg", 4), yat(6), 1)
                send(sg.at[:, k], sg.at[:, k], ("sgm",), mate, 1)

    def x_sends(k):
        for e in (2, 1, 3):
            send(part.at[k, (x + e) % NX], xin.at[k, e - 1], ("xin", k), xat(e))

    def x_sum(k):
        wait(xin.at[k], ("xin", k))
        total = part[k, x].astype(F32)
        for n in range(3):
            total += xin[k, n].astype(F32)
        return total

    def z_send(k):
        if k:
            zout[k] = x_sum(k).astype(BF16)
            send(zout.at[k], zin.at[k], ("zin",), zat(NZ - k))

    def group(k, first):
        q = zf[k, :, 0:64, :].reshape(256, 256)
        h = xf[k].reshape(256, 256)
        stat = jnp.sum(zf[k, :, 64:72, :].astype(F32), axis=0)
        score = nt(kb[...], q)
        prob = jnp.exp(score * SCALE - (SHIFT + stat[0:1]))
        grad = prob * (nt(vb[...], h) - stat[1:2]) * SCALE
        prob = prob.astype(BF16)
        dv_new = nn(prob, h)
        dk_new = nn(grad.astype(BF16), q)
        if first:
            dv[...] = dv_new
            dk[...] = dk_new
        else:
            dv[...] += dv_new
            dk[...] += dk_new
        dq = nn(jnp.transpose(grad).astype(BF16), kb[...])
        part[k] = dq.astype(BF16).reshape(4, 64, 256)

    def work(k, first=False):
        phase(f"group{k}")
        zf_end(k)
        group(k, first)
        if k not in (0, 1, 7):
            x_sends(k)

    phase("spsend")
    zf_z(0)
    xf_z(0, 0)
    zf_x(0)

    phase("step1")
    for e in (1, 3):
        wait(xf.at[0, xs(e)], ("xfx", e))
        xf_z(0, e)
    for k in (1, 7):
        zf_z(k)
    sg_in(2, 6)
    wait(xf.at[0, xs(2)], ("xfx", 2))
    xf_z(0, 2)
    for k in (1, 7):
        xf_z(k, 0)
    for k in (1, 7):
        zf_x(k)
    phase("step2")
    for e in (1, 3):
        xf_z(1, e)
        xf_z(7, e)
    for k in (2, 6):
        zf_z(k)
        xf_z(k, 0)
    for k in (1, 7):
        xf_z(k, 2)
    for k in (2, 6):
        zf_x(k)
    sg_in(1, 7, 3, 5, 4)
    nza[0] = nzs[z]
    wait(nza.at[1:8], ("nza",))
    nyb[c, y] = nza[...]
    for k in (4, 3, 5, 2, 6, 1, 7):
        send(nza, nyb.at[c, y], ("nyb",), yat(k))
    send(nza, nyb.at[c, y], ("nybm",), mate)
    phase("kproj")

    @pl.when(c == 0)
    def _():
        wait(sg.at[1, 0], ("sg0",))
        wait(sg.at[:, 1:8], ("sgm",))

    loads["k"].wait()
    kb[...] = nn(sg[...].reshape(256, 2048), wk[...]).astype(BF16)
    phase("vproj")
    loads["v"].wait()
    vb[...] = nn(sg[...].reshape(256, 2048), wv[...]).astype(BF16)
    phase("step3")
    for e in (1, 3):
        xf_z(2, e)
        xf_z(6, e)
    for k in (3, 5):
        zf_z(k)
        xf_z(k, 0)
    for k in (2, 6):
        xf_z(k, 2)
    for k in (3, 5):
        zf_x(k)
    work(1, True)
    work(7)
    phase("step4")
    for e in (1, 3):
        xf_z(3, e)
        xf_z(5, e)
    zf_z(4)
    zf_x(4)
    for k in (3, 5):
        xf_z(k, 2)
    for k in (1, 7):
        send(part.at[k], near.at[k // 7], ("near", k), zat(NZ - k))
    phase("nyb")
    wait(nyb.at[0, 0:7], ("nyb",))
    for k in range(1, NY):
        send(nyb.at[c, (y + k) % NY], nyb.at[c, (y + k) % NY], ("nybm",), mate)
    work(2)
    work(6)
    work(0)
    phase("xf4")
    for e in range(4):
        xf_z(4, e)
    work(3)
    work(5)
    work(4)

    phase("gmat1")
    dkb = dk[...].astype(BF16)
    dvb = dv[...].astype(BF16)

    def gmat(half):
        lo = 128 * half
        for f in range(4):
            cols = pl.ds(512 * f, 512)
            gout[half, :, :, cols] = (
                (nt(dkb[lo : lo + 128], wk[cols, :]) + nt(dvb[lo : lo + 128], wv[cols, :]))
                .astype(BF16)
                .reshape(8, 16, 512)
            )

    gmat(0)
    phase("zsend2")
    z_send(2)
    phase("gmat0")
    gmat(1)
    send(gout.at[1 - c], gin, ("gm",), mate)
    phase("zsend6")
    z_send(6)
    phase("near")
    wait(near.at[0], ("near", 1))
    wait(near.at[1], ("near", 7))
    part[0] = (part[0].astype(F32) + near[0].astype(F32) + near[1].astype(F32)).astype(BF16)
    x_sends(0)
    phase("zsend3")
    z_send(3)
    phase("zsend5")
    z_send(5)
    phase("zsend4")
    z_send(4)
    phase("nrt")
    wait(nyb.at[0], ("nybm",))
    for s in range(16):
        rows = nyb[s % 2, s // 2].astype(F32)
        for k in range(NZ):
            nr[k, 4 * s : 4 * s + 4] = rows[k]
    for j in range(4):
        pair = nr[2 * j : 2 * j + 2].reshape(128, 256)
        nrt[:, 128 * j : 128 * j + 128] = pair.T.astype(BF16)
    phase("gsum")
    wait(gin, ("gm",))
    for k in (4, 3, 5, 1, 7):
        gsum[k] = (gout[c, k].astype(F32) + gin[k].astype(F32)).astype(BF16)
    send(gsum.at[4], gmid.at[2], ("gmid",), yat((NY - 2 * way) % NY))
    send(gsum.at[3], gmid.at[0], ("gmid",), yat(7))
    send(gsum.at[5], gmid.at[1], ("gmid",), yat(1))
    send(gsum.at[1], grecv.at[1], ("g",), yat(7))
    send(gsum.at[7], grecv.at[7], ("g",), yat(1))
    phase("qflat")
    total = x_sum(0)
    wait(zin.at[2:7], ("zin",))
    for k in range(2, 7):
        total += zin[k].astype(F32)
    qflat = total.astype(BF16)
    qz[0] = qflat

    for k in (4, 3, 5, 2, 6, 1, 7):
        send(qz.at[0], qz.at[k], ("qz",), zat(k))

    phase("ng")
    for f in range(2):
        halves = [nt(qflat, wq[1024 * g + 512 * f : 1024 * g + 512 * f + 512, :]) for g in range(2)]
        for s in range(16):
            nout[s % 2, s // 2, :, 512 * f : 512 * f + 512] = jnp.concatenate(
                [half[4 * s : 4 * s + 4] for half in halves], axis=0
            ).astype(BF16)
    send(nout.at[1 - c], nin, ("nm",), mate)
    phase("gmid")
    wait(gmid, ("gmid",))
    for k, n in ((2, 0), (6, 1)):
        mid = jnp.where(c == n, gmid[2].astype(F32), 0.0) + gmid[n].astype(F32)
        gsum[k] = (gout[c, k].astype(F32) + gin[k].astype(F32) + mid).astype(BF16)
        send(gsum.at[k], grecv.at[k], ("g",), yat(NY - k))
    phase("nsum")
    wait(nin, ("nm",))
    nsum[...] = (nout[c].astype(F32) + nin[...].astype(F32)).astype(BF16)
    for k in (4, 3, 5, 2, 6, 1, 7):
        send(nsum.at[(y + NY - k) % NY], nrecv.at[k], ("n",), yat(NY - k))

    phase("wmat")
    wait(qz.at[1:8], ("qz",))
    wsum = nn(nrt[...], qz[...].reshape(512, 256))
    wpart[...] = wsum.astype(BF16).reshape(4, 64, 256)
    for e in (2, 1, 3):
        send(wpart.at[(x + e) % NX], win.at[e], ("w",), xat(e))

    phase("gfin")
    wait(grecv.at[0:4], ("g",))
    total = gout[c, 0].astype(F32) + gin[0].astype(F32)
    for k in (1, 2, 6, 7):
        total += grecv[k].astype(F32)
    sgrad_ref[...] = total

    phase("nfin")
    wait(nrecv.at[1:8], ("n",))
    total = nsum[y].astype(F32)
    for k in range(1, NY):
        total += nrecv[k].astype(F32)
    scaled = jnp.concatenate([total[0:4], total[4:8]], axis=1) * gain
    mean = jnp.mean(scaled * target, axis=1, keepdims=True)
    tgrad_ref[...] = inverse * scaled - target * (inverse * inverse * inverse) * mean

    phase("wfin")
    wait(win.at[1:4], ("w",))
    total = wpart[x].astype(F32)
    for e in range(1, NX):
        total += win[e].astype(F32)
    wgrad_ref[...] = total

    phase("sendwait")
    def sent_all(sem):
        whole = units.at[0 : sent[sem]]
        pltpu.make_async_remote_copy(
            src_ref=whole, dst_ref=whole, send_sem=ssem.at[sem], recv_sem=rsem.at[0],
            device_id=mate, device_id_type=MESH,
        ).wait_send()

    sent_all(0)

    @pl.when(c == 1)
    def _():
        sent_all(1)

    phase(None)
    assert max(sent) <= UNITS and len(names) <= RECVS, (sent[0], len(names))


def finish(a_ref, b_ref, c_ref, oa_ref, ob_ref, oc_ref):
    oa_ref[...] = a_ref[...]
    ob_ref[...] = b_ref[...]
    oc_ref[...] = c_ref[...]


def body(tr, sr, gain, wq, wk, wv, wo, saved, offset, og):
    vm = pl.BlockSpec(memory_space=pltpu.VMEM)
    hb = pl.BlockSpec(memory_space=pl.ANY)

    def buf(*shape, dtype=BF16):
        return pltpu.VMEM(shape, dtype)

    outs = (
        jax.ShapeDtypeStruct((4, 2048), F32),
        jax.ShapeDtypeStruct((16, 2048), F32),
        jax.ShapeDtypeStruct((64, 256), F32),
    )
    results = pl.pallas_call(
        kernel,
        out_shape=tuple(pltpu.VMEM(o.shape, o.dtype) for o in outs),
        in_specs=[hb] * 10,
        out_specs=(vm, vm, vm),
        scratch_shapes=[
            buf(4, 2048), buf(16, 128), buf(64, 256), buf(1, 64), buf(4, 2048),
            buf(2, 8, 8, 2048), buf(64, 2048, dtype=F32), buf(64, 2048, dtype=F32),
            buf(8, 4, 256), buf(8, 4, 256), buf(2, 8, 8, 4, 256),
            buf(8, 64, 256, dtype=F32), buf(256, 512), buf(2, 8, 16, 2048),
            buf(2048, 256), buf(2048, 256), buf(2048, 256), buf(256, 2048),
            buf(8, 4, 72, 256), buf(8, 4, 64, 256),
            buf(256, 256), buf(256, 256),
            buf(256, 256, dtype=F32), buf(256, 256, dtype=F32),
            buf(8, 4, 64, 256), buf(2, 4, 64, 256),
            buf(8, 3, 64, 256),
            buf(8, 64, 256), buf(8, 64, 256),
            buf(8, 64, 256), buf(4, 64, 256), buf(4, 64, 256),
            buf(2, 8, 16, 2048), buf(8, 16, 2048), buf(8, 16, 2048), buf(3, 16, 2048), buf(8, 16, 2048),
            buf(2, 8, 8, 1024), buf(8, 8, 1024), buf(8, 8, 1024), buf(8, 8, 1024),
            buf(UNITS, 4, 256),
            pltpu.SemaphoreType.DMA((2,)),
            pltpu.SemaphoreType.DMA((RECVS,)),
            pltpu.SemaphoreType.DMA((10,)),
        ],
        compiler_params=pltpu.CompilerParams(
            collective_id=0, has_side_effects=True, vmem_limit_bytes=60 * 1024 * 1024
        ),
    )(tr, sr, gain.reshape(16, 128), wq, wk, wv, wo, saved, offset.reshape(1, 64), og)
    return pl.pallas_call(
        finish, out_shape=outs, in_specs=[vm, vm, vm], out_specs=(vm, vm, vm)
    )(*[pltpu.with_memory_space_constraint(r, pltpu.VMEM) for r in results])


def solution(mesh):
    split = Mesh(mesh.devices.reshape(NZ, NX, mesh.shape["tp"]), ("sp_0", "sp_1", "tp"))
    placed = (
        P(SP_TP, None), P(SP_TP, None), P(), P(None, "tp"), P(None, "tp"), P(None, "tp"),
        P("tp", None), P(SP, "tp"), P(SP, "tp"), P(SP_TP, None),
    )
    return jax.shard_map(
        body,
        mesh=split,
        in_specs=placed,
        out_specs=(P(SP_TP, None), P(SP_TP, None), P(SP, "tp")),
        check_vma=False,
    )
```

```python
import math

import jax
import jax.numpy as jnp
from jax import lax
from jax.experimental import pallas as pl
from jax.experimental.pallas import tpu as pltpu
from jax.sharding import Mesh
from jax.sharding import PartitionSpec as P

SP = ("sp_0", "sp_1")
SP_TP = ("sp_0", "sp_1", "tp")
EPSILON = 1e-06
SCALE = 256 ** (-0.5)
SHIFT = math.log(8192)
MESH = pl.DeviceIdType.MESH
F32 = jnp.float32
BF16 = jnp.bfloat16
NZ, NX, NY = 8, 4, 8
UNIT = 2048
UNITS = 4096
RECVS = 112


def nt(left, right):
    return lax.dot_general(left, right, (((1,), (1,)), ((), ())), preferred_element_type=F32)


def nn(left, right):
    return lax.dot_general(left, right, (((1,), (0,)), ((), ())), preferred_element_type=F32)


def kernel(
    tr_hbm, sr_hbm, gain_hbm, wq_hbm, wk_hbm, wv_hbm, wo_hbm, saved_hbm, off_hbm, og_hbm,
    tgrad_ref, sgrad_ref, wgrad_ref,
    tr, gn, sv, of, og,
    tg, xn, xo, nzs, nza, nyb, nr, nrt, nxs, nxa, nyx, nrx, nrtx, sg, wq, wk, wv, wo, zf, xf, kb, vb, dk, dv,
    part, near, xin, zout, zin,
    qz, qx, wz, wzin, wpart, win,
    gout, gin, gsum, gmid, grecv, nout, nin, nsum, nrecv,
    units, ssem, rsem, lsem,
):
    z = lax.axis_index("sp_0")
    x = lax.axis_index("sp_1")
    t = lax.axis_index("tp")
    y = t // 2
    c = t % 2
    way = 1 - 2 * c

    def zat(k):
        return ((z + k) % NZ, x, t)

    def xat(k):
        return (z, (x + k) % NX, t)

    def yat(k):
        return (z, x, ((y + k) % NY) * 2 + c)

    mate = (z, x, t + way)
    names = {}
    sent = [0, 0]
    scope = [None]

    def phase(name):
        if scope[0] is not None:
            scope[0].__exit__(None, None, None)
        scope[0] = jax.named_scope(name) if name else None
        if name:
            scope[0].__enter__()

    def size(ref):
        return math.prod(ref.shape) * 2

    def slot_of(name):
        if name not in names:
            names[name] = len(names)
        return names[name]

    def send(src, dst, name, dev, sem=0):
        assert size(src) % UNIT == 0
        sent[sem] += size(src) // UNIT
        pltpu.make_async_remote_copy(
            src_ref=src, dst_ref=dst, send_sem=ssem.at[sem], recv_sem=rsem.at[slot_of(name)],
            device_id=dev, device_id_type=MESH,
        ).start()

    def wait(dst, name):
        pltpu.make_async_remote_copy(
            src_ref=dst, dst_ref=dst, send_sem=ssem.at[0], recv_sem=rsem.at[slot_of(name)],
            device_id=mate, device_id_type=MESH,
        ).wait_recv()

    phase("start")
    barrier = pltpu.get_barrier_semaphore()
    peers = [mate] + [yat(k) for k in range(1, NY)] + [xat(k) for k in range(1, NX)]
    peers += [zat(k) for k in range(1, NZ)]
    for dev in peers:
        pl.semaphore_signal(barrier, inc=1, device_id=dev, device_id_type=MESH)

    loads = {}
    for k, (name, src, dst) in enumerate(
        (
            ("tr", tr_hbm, tr), ("og", og_hbm, og), ("gn", gain_hbm, gn), ("sr", sr_hbm, sg.at[c, 0]),
            ("of", off_hbm, of), ("sv", saved_hbm, sv),
            ("q", wq_hbm, wq), ("o", wo_hbm, wo), ("k", wk_hbm, wk), ("v", wv_hbm, wv),
        )
    ):
        loads[name] = pltpu.make_async_copy(src, dst, lsem.at[k])
        loads[name].start()

    for name in ("tr", "og", "gn"):
        loads[name].wait()
    gain = gn[...].astype(F32)
    gain = jnp.concatenate([gain[s : s + 1] for s in range(16)], axis=1)
    target = tr[...].astype(F32)
    inverse = lax.rsqrt(jnp.mean(target * target, axis=1, keepdims=True) + EPSILON)
    normed = target * inverse * gain
    tg[c, y] = jnp.concatenate([normed, og[...].astype(F32)], axis=0).astype(BF16)
    for f in range(NZ):
        nzs[f] = normed[:, 256 * f : 256 * f + 256].astype(BF16)
    for f in range(NX):
        nxs[f] = jnp.concatenate(
            [normed[:, 256 * g + 64 * f : 256 * g + 64 * f + 64] for g in range(NZ)], axis=1
        ).astype(BF16)
    phase("barrier")
    pl.semaphore_wait(barrier, len(peers))

    phase("tgwait")
    loads["sr"].wait()
    send(sg.at[c, 0], sg.at[c, 0], ("sg0",), mate)

    def tg_of(k):
        return tg.at[c, (y + NY - k) % NY]

    for k in (4, 3, 5, 2, 6, 1, 7):
        send(tg_of(0), tg_of(0), ("tg", k), yat(k))
    send(tg_of(0), tg_of(0), ("tgm",), mate)
    for k in range(1, NZ):
        send(nzs.at[(z + k) % NZ], nza.at[k], ("nza",), zat(k))
    for e in range(1, NX):
        send(nxs.at[(x + e) % NX], nxa.at[x], ("nxa",), xat(e))
    for k in (3, 5, 2, 6, 4, 1, 7):
        wait(tg_of(k), ("tg", k))
        send(tg_of(k), tg_of(k), ("tgm",), mate)

    @pl.when(c == 1)
    def _():
        wait(sg.at[0, 0], ("sg0",))
        for k in (2, 6, 1, 7):
            send(sg.at[:, 0], sg.at[:, k], ("sg", k), yat(k), 1)

    phase("tgmate")
    wait(tg.at[1 - c], ("tgm",))

    phase("qproj")
    for s in range(16):
        rows = tg[s % 2, s // 2].astype(F32)
        xn[4 * s : 4 * s + 4] = rows[0:4]
        xo[4 * s : 4 * s + 4] = rows[4:8]
    loads["o"].wait()
    hgrad = nt(xo[...].astype(BF16), wo[...]).astype(BF16)
    xf[0, x] = hgrad
    for e in (2, 1, 3):
        send(xf.at[0, x], xf.at[0, x], ("xfx", e), xat(e))
    loads["q"].wait()
    zf[0, x, 0:64] = nn(xn[...].astype(BF16), wq[...]).astype(BF16)
    loads["sv"].wait()
    loads["of"].wait()
    deltas = jnp.sum(hgrad.astype(F32) * sv[...].astype(F32), axis=1, keepdims=True)
    deltas = jnp.broadcast_to(deltas, (64, 128)).T[0:16]
    first = lax.broadcasted_iota(jnp.int32, (16, 64), 0) == 0
    both = jnp.where(first, of[...].astype(F32), deltas).astype(BF16)
    place = lax.broadcasted_iota(jnp.int32, (64, 256), 1) == x * 64 + lax.broadcasted_iota(
        jnp.int32, (64, 256), 0
    )
    zf[0, x, 64:72] = nn(both, place.astype(F32).astype(BF16))[0:8].astype(BF16)

    def xs(e):
        return (x + NX - e) % NX

    def zf_x(k):
        for e in (2, 1, 3):
            send(zf.at[k, x], zf.at[k, x], ("zfx", k, e), xat(e))

    def zf_z(k):
        if k:
            wait(zf.at[k, x], ("zfz", k))
        if k <= 3:
            send(zf.at[k, x], zf.at[k + 1, x], ("zfz", k + 1), zat(1))
        if k == 0 or k >= 6:
            send(zf.at[k, x], zf.at[(k - 1) % NZ, x], ("zfz", (k - 1) % NZ), zat(7))

    def zf_end(k):
        for e in (1, 3, 2):
            wait(zf.at[k, xs(e)], ("zfx", k, e))

    def xf_z(k, e):
        if k:
            wait(xf.at[k, xs(e)], ("xfz", k, e))
        if k <= 2 or (k == 3 and e % 2 == 0):
            send(xf.at[k, xs(e)], xf.at[k + 1, xs(e)], ("xfz", k + 1, e), zat(1))
        if k == 0 or k >= 6 or (k == 5 and e % 2 == 1):
            send(xf.at[k, xs(e)], xf.at[(k - 1) % NZ, xs(e)], ("xfz", (k - 1) % NZ, e), zat(7))

    def sg_in(*ks):
        @pl.when(c == 1)
        def _():
            for k in ks:
                wait(sg.at[:, k], ("sg", k))
                if k == 2:
                    send(sg.at[:, 2], sg.at[:, 3], ("sg", 3), yat(1), 1)
                    send(sg.at[0, 2], sg.at[0, 4], ("sg", 4), yat(2), 1)
                if k == 6:
                    send(sg.at[:, 6], sg.at[:, 5], ("sg", 5), yat(7), 1)
                    send(sg.at[1, 6], sg.at[1, 4], ("sg", 4), yat(6), 1)
                send(sg.at[:, k], sg.at[:, k], ("sgm",), mate, 1)

    def x_sends(k):
        for e in (2, 1, 3):
            send(part.at[k, (x + e) % NX], xin.at[k, e - 1], ("xin", k), xat(e))

    def x_sum(k):
        wait(xin.at[k], ("xin", k))
        total = part[k, x].astype(F32)
        for n in range(3):
            total += xin[k, n].astype(F32)
        return total

    def z_send(k):
        if k:
            zout[k] = x_sum(k).astype(BF16)
            send(zout.at[k], zin.at[k], ("zin",), zat(NZ - k))

    def group(k, first):
        q = zf[k, :, 0:64, :].reshape(256, 256)
        h = xf[k].reshape(256, 256)
        stat = jnp.sum(zf[k, :, 64:72, :].astype(F32), axis=0)
        score = nt(kb[...], q)
        prob = jnp.exp(score * SCALE - (SHIFT + stat[0:1]))
        grad = prob * (nt(vb[...], h) - stat[1:2]) * SCALE
        prob = prob.astype(BF16)
        dv_new = nn(prob, h)
        dk_new = nn(grad.astype(BF16), q)
        if first:
            dv[...] = dv_new
            dk[...] = dk_new
        else:
            dv[...] += dv_new
            dk[...] += dk_new
        dq = nn(jnp.transpose(grad).astype(BF16), kb[...])
        part[k] = dq.astype(BF16).reshape(4, 64, 256)

    def work(k, first=False):
        phase(f"group{k}")
        zf_end(k)
        group(k, first)
        if k not in (0, 1, 7):
            x_sends(k)

    phase("spsend")
    zf_z(0)
    xf_z(0, 0)
    zf_x(0)

    phase("step1")
    for e in (1, 3):
        wait(xf.at[0, xs(e)], ("xfx", e))
        xf_z(0, e)
    for k in (1, 7):
        zf_z(k)
    sg_in(2, 6)
    wait(xf.at[0, xs(2)], ("xfx", 2))
    xf_z(0, 2)
    for k in (1, 7):
        xf_z(k, 0)
    for k in (1, 7):
        zf_x(k)
    phase("step2")
    for e in (1, 3):
        xf_z(1, e)
        xf_z(7, e)
    for k in (2, 6):
        zf_z(k)
        xf_z(k, 0)
    for k in (1, 7):
        xf_z(k, 2)
    for k in (2, 6):
        zf_x(k)
    sg_in(1, 7, 3, 5, 4)
    nza[0] = nzs[z]
    wait(nza.at[1:8], ("nza",))
    nyb[c, y] = nza[...]
    nxa[x] = nxs[x]
    wait(nxa.at[0:3], ("nxa",))
    nyx[c, y] = nxa[...]
    for k in (4, 3, 5, 2, 6, 1, 7):
        send(nza, nyb.at[c, y], ("nyb",), yat(k))
    send(nza, nyb.at[c, y], ("nybm",), mate)
    for k in (4, 3, 5, 2, 6, 1, 7):
        send(nxa, nyx.at[c, y], ("nyx",), yat(k))
    send(nxa, nyx.at[c, y], ("nyxm",), mate)
    phase("kproj")

    @pl.when(c == 0)
    def _():
        wait(sg.at[1, 0], ("sg0",))
        wait(sg.at[:, 1:8], ("sgm",))

    loads["k"].wait()
    kb[...] = nn(sg[...].reshape(256, 2048), wk[...]).astype(BF16)
    phase("vproj")
    loads["v"].wait()
    vb[...] = nn(sg[...].reshape(256, 2048), wv[...]).astype(BF16)
    phase("step3")
    for e in (1, 3):
        xf_z(2, e)
        xf_z(6, e)
    for k in (3, 5):
        zf_z(k)
        xf_z(k, 0)
    for k in (2, 6):
        xf_z(k, 2)
    for k in (3, 5):
        zf_x(k)
    work(1, True)
    work(7)
    phase("step4")
    for e in (1, 3):
        xf_z(3, e)
        xf_z(5, e)
    zf_z(4)
    zf_x(4)
    for k in (3, 5):
        xf_z(k, 2)
    for k in (1, 7):
        send(part.at[k], near.at[k // 7], ("near", k), zat(NZ - k))
    work(2)
    work(6)
    work(0)
    phase("xf4")
    for e in range(4):
        xf_z(4, e)
    work(3)
    work(5)
    work(4)

    phase("gmat1")
    dkb = dk[...].astype(BF16)
    dvb = dv[...].astype(BF16)

    def gmat(half):
        lo = 128 * half
        for f in range(4):
            cols = pl.ds(512 * f, 512)
            gout[half, :, :, cols] = (
                (nt(dkb[lo : lo + 128], wk[cols, :]) + nt(dvb[lo : lo + 128], wv[cols, :]))
                .astype(BF16)
                .reshape(8, 16, 512)
            )

    gmat(0)
    phase("zsend2")
    z_send(2)
    phase("gmat0")
    gmat(1)
    send(gout.at[1 - c], gin, ("gm",), mate)
    phase("zsend6")
    z_send(6)
    phase("nyb")
    wait(nyb.at[0, 0:7], ("nyb",))
    for k in range(1, NY):
        send(nyb.at[c, (y + k) % NY], nyb.at[c, (y + k) % NY], ("nybm",), mate)
    wait(nyx.at[0, 0:7], ("nyx",))
    for k in range(1, NY):
        send(nyx.at[c, (y + k) % NY], nyx.at[c, (y + k) % NY], ("nyxm",), mate)
    phase("near")
    wait(near.at[0], ("near", 1))
    wait(near.at[1], ("near", 7))
    part[0] = (part[0].astype(F32) + near[0].astype(F32) + near[1].astype(F32)).astype(BF16)
    x_sends(0)
    phase("zsend3")
    z_send(3)
    phase("zsend5")
    z_send(5)
    phase("zsend4")
    z_send(4)
    phase("nrt")
    wait(nyb.at[0], ("nybm",))
    for s in range(16):
        rows = nyb[s % 2, s // 2].astype(F32)
        for k in range(NZ):
            nr[k, 4 * s : 4 * s + 4] = rows[k]
    for j in range(4):
        pair = nr[2 * j : 2 * j + 2].reshape(128, 256)
        nrt[:, 128 * j : 128 * j + 128] = pair.T.astype(BF16)
    wait(nyx.at[0], ("nyxm",))
    for s in range(16):
        rows = nyx[s % 2, s // 2].astype(F32)
        for k in range(NX):
            nrx[k, 4 * s : 4 * s + 4] = rows[k]
    for j in range(2):
        pair = nrx[2 * j : 2 * j + 2].reshape(128, 512)
        nrtx[:, 128 * j : 128 * j + 128] = pair.T.astype(BF16)
    phase("gsum")
    wait(gin, ("gm",))
    for k in (4, 3, 5, 1, 7):
        gsum[k] = (gout[c, k].astype(F32) + gin[k].astype(F32)).astype(BF16)
    send(gsum.at[4], gmid.at[2], ("gmid",), yat((NY - 2 * way) % NY))
    send(gsum.at[3], gmid.at[0], ("gmid",), yat(7))
    send(gsum.at[5], gmid.at[1], ("gmid",), yat(1))
    send(gsum.at[1], grecv.at[1], ("g",), yat(7))
    send(gsum.at[7], grecv.at[7], ("g",), yat(1))
    phase("qflat")
    total = x_sum(0)
    wait(zin.at[2:7], ("zin",))
    for k in range(2, 7):
        total += zin[k].astype(F32)
    qflat = total.astype(BF16)
    qz[0] = qflat[:, 0:128]
    qx[x] = qflat[:, 128:256]
    for e in (2, 1, 3):
        send(qx.at[x], qx.at[x], ("qx",), xat(e))
    for k in (4, 3, 5, 2, 6, 1, 7):
        send(qz.at[0], qz.at[k], ("qz",), zat(k))

    phase("ng")
    for f in range(2):
        halves = [nt(qflat, wq[1024 * g + 512 * f : 1024 * g + 512 * f + 512, :]) for g in range(2)]
        for s in range(16):
            nout[s % 2, s // 2, :, 512 * f : 512 * f + 512] = jnp.concatenate(
                [half[4 * s : 4 * s + 4] for half in halves], axis=0
            ).astype(BF16)
    send(nout.at[1 - c], nin, ("nm",), mate)
    phase("gmid")
    wait(gmid, ("gmid",))
    for k, n in ((2, 0), (6, 1)):
        mid = jnp.where(c == n, gmid[2].astype(F32), 0.0) + gmid[n].astype(F32)
        gsum[k] = (gout[c, k].astype(F32) + gin[k].astype(F32) + mid).astype(BF16)
        send(gsum.at[k], grecv.at[k], ("g",), yat(NY - k))
    phase("nsum")
    wait(nin, ("nm",))
    nsum[...] = (nout[c].astype(F32) + nin[...].astype(F32)).astype(BF16)
    for k in (4, 3, 5, 2, 6, 1, 7):
        send(nsum.at[(y + NY - k) % NY], nrecv.at[k], ("n",), yat(NY - k))

    phase("wmat2")
    wait(qx.at[0:3], ("qx",))
    wz[...] = nn(nrtx[...], qx[...].reshape(256, 128)).astype(BF16).reshape(8, 64, 128)
    for k in (4, 3, 5, 2, 6, 1, 7):
        send(wz.at[(z + k) % NZ], wzin.at[k], ("wz",), zat(k))
    phase("wmat")
    wait(qz.at[1:8], ("qz",))
    wpart[...] = nn(nrt[...], qz[...].reshape(512, 128)).astype(BF16).reshape(4, 64, 128)
    for e in (2, 1, 3):
        send(wpart.at[(x + e) % NX], win.at[e], ("w",), xat(e))

    phase("gfin")
    wait(grecv.at[0:4], ("g",))
    total = gout[c, 0].astype(F32) + gin[0].astype(F32)
    for k in (1, 2, 6, 7):
        total += grecv[k].astype(F32)
    sgrad_ref[...] = total

    phase("nfin")
    wait(nrecv.at[1:8], ("n",))
    total = nsum[y].astype(F32)
    for k in range(1, NY):
        total += nrecv[k].astype(F32)
    scaled = jnp.concatenate([total[0:4], total[4:8]], axis=1) * gain
    mean = jnp.mean(scaled * target, axis=1, keepdims=True)
    tgrad_ref[...] = inverse * scaled - target * (inverse * inverse * inverse) * mean

    phase("wfin")
    wait(win.at[1:4], ("w",))
    total = wpart[x].astype(F32)
    for e in range(1, NX):
        total += win[e].astype(F32)
    wgrad_ref[:, 0:128] = total
    wait(wzin.at[1:8], ("wz",))
    total = wz[z].astype(F32)
    for k in range(1, NZ):
        total += wzin[k].astype(F32)
    wgrad_ref[:, 128:256] = total

    phase("sendwait")
    def sent_all(sem):
        whole = units.at[0 : sent[sem]]
        pltpu.make_async_remote_copy(
            src_ref=whole, dst_ref=whole, send_sem=ssem.at[sem], recv_sem=rsem.at[0],
            device_id=mate, device_id_type=MESH,
        ).wait_send()

    sent_all(0)

    @pl.when(c == 1)
    def _():
        sent_all(1)

    phase(None)
    assert max(sent) <= UNITS and len(names) <= RECVS, (sent[0], len(names))


def finish(a_ref, b_ref, c_ref, oa_ref, ob_ref, oc_ref):
    oa_ref[...] = a_ref[...]
    ob_ref[...] = b_ref[...]
    oc_ref[...] = c_ref[...]


def body(tr, sr, gain, wq, wk, wv, wo, saved, offset, og):
    vm = pl.BlockSpec(memory_space=pltpu.VMEM)
    hb = pl.BlockSpec(memory_space=pl.ANY)

    def buf(*shape, dtype=BF16):
        return pltpu.VMEM(shape, dtype)

    outs = (
        jax.ShapeDtypeStruct((4, 2048), F32),
        jax.ShapeDtypeStruct((16, 2048), F32),
        jax.ShapeDtypeStruct((64, 256), F32),
    )
    results = pl.pallas_call(
        kernel,
        out_shape=tuple(pltpu.VMEM(o.shape, o.dtype) for o in outs),
        in_specs=[hb] * 10,
        out_specs=(vm, vm, vm),
        scratch_shapes=[
            buf(4, 2048), buf(16, 128), buf(64, 256), buf(1, 64), buf(4, 2048),
            buf(2, 8, 8, 2048), buf(64, 2048, dtype=F32), buf(64, 2048, dtype=F32),
            buf(8, 4, 256), buf(8, 4, 256), buf(2, 8, 8, 4, 256),
            buf(8, 64, 256, dtype=F32), buf(256, 512),
            buf(4, 4, 512), buf(4, 4, 512), buf(2, 8, 4, 4, 512), buf(4, 64, 512, dtype=F32), buf(512, 256),
            buf(2, 8, 16, 2048),
            buf(2048, 256), buf(2048, 256), buf(2048, 256), buf(256, 2048),
            buf(8, 4, 72, 256), buf(8, 4, 64, 256),
            buf(256, 256), buf(256, 256),
            buf(256, 256, dtype=F32), buf(256, 256, dtype=F32),
            buf(8, 4, 64, 256), buf(2, 4, 64, 256),
            buf(8, 3, 64, 256),
            buf(8, 64, 256), buf(8, 64, 256),
            buf(8, 64, 128), buf(4, 64, 128), buf(8, 64, 128), buf(8, 64, 128), buf(4, 64, 128), buf(4, 64, 128),
            buf(2, 8, 16, 2048), buf(8, 16, 2048), buf(8, 16, 2048), buf(3, 16, 2048), buf(8, 16, 2048),
            buf(2, 8, 8, 1024), buf(8, 8, 1024), buf(8, 8, 1024), buf(8, 8, 1024),
            buf(UNITS, 4, 256),
            pltpu.SemaphoreType.DMA((2,)),
            pltpu.SemaphoreType.DMA((RECVS,)),
            pltpu.SemaphoreType.DMA((10,)),
        ],
        compiler_params=pltpu.CompilerParams(
            collective_id=0, has_side_effects=True, vmem_limit_bytes=60 * 1024 * 1024
        ),
    )(tr, sr, gain.reshape(16, 128), wq, wk, wv, wo, saved, offset.reshape(1, 64), og)
    return pl.pallas_call(
        finish, out_shape=outs, in_specs=[vm, vm, vm], out_specs=(vm, vm, vm)
    )(*[pltpu.with_memory_space_constraint(r, pltpu.VMEM) for r in results])


def solution(mesh):
    split = Mesh(mesh.devices.reshape(NZ, NX, mesh.shape["tp"]), ("sp_0", "sp_1", "tp"))
    placed = (
        P(SP_TP, None), P(SP_TP, None), P(), P(None, "tp"), P(None, "tp"), P(None, "tp"),
        P("tp", None), P(SP, "tp"), P(SP, "tp"), P(SP_TP, None),
    )
    return jax.shard_map(
        body,
        mesh=split,
        in_specs=placed,
        out_specs=(P(SP_TP, None), P(SP_TP, None), P(SP, "tp")),
        check_vma=False,
    )
```

```python
import functools
import math

import jax
import jax.numpy as jnp
from jax import lax
from jax.experimental import pallas as pl
from jax.experimental.pallas import tpu as pltpu
from jax.sharding import Mesh
from jax.sharding import PartitionSpec as P

SP = ("sp_0", "sp_1")
SP_TP = ("sp_0", "sp_1", "tp")
EPSILON = 1e-06
SCALE = 256 ** (-0.5)
SHIFT = math.log(8192)
MESH = pl.DeviceIdType.MESH
F32 = jnp.float32
BF16 = jnp.bfloat16
NZ, NX, NY = 8, 4, 8
UNIT = 2048
UNITS = 4096
RECVS = 112


def nt(left, right):
    return lax.dot_general(left, right, (((1,), (1,)), ((), ())), preferred_element_type=F32)


def nn(left, right):
    return lax.dot_general(left, right, (((1,), (0,)), ((), ())), preferred_element_type=F32)


def kernel(
    tr_hbm, sr_hbm, gain_hbm, wq_hbm, wk_hbm, wv_hbm, wo_hbm, saved_hbm, off_hbm, og_hbm,
    tgrad_ref, sgrad_ref, wgrad_ref,
    tr, gn, sv, of, og,
    tg, xn, xo, nzs, nza, nyb, nr, nrt, nxs, nxa, nyx, nrx, nrtx, sg, wq, wk, wv, wo, zf, xf, kb, vb, dk, dv,
    part, near, reli, relo, xin, zout, zin,
    qz, qx, wz, wzin, wpart, win,
    gout, gin, gsum, gmid, grecv, nout, nin, nsum, nrecv,
    units, ssem, rsem, lsem,
):
    z = lax.axis_index("sp_0")
    x = lax.axis_index("sp_1")
    t = lax.axis_index("tp")
    y = t // 2
    c = t % 2
    way = 1 - 2 * c

    def zat(k):
        return ((z + k) % NZ, x, t)

    def xat(k):
        return (z, (x + k) % NX, t)

    def yat(k):
        return (z, x, ((y + k) % NY) * 2 + c)

    mate = (z, x, t + way)
    names = {}
    sent = [0, 0]
    scope = [None]

    def phase(name):
        if scope[0] is not None:
            scope[0].__exit__(None, None, None)
        scope[0] = jax.named_scope(name) if name else None
        if name:
            scope[0].__enter__()

    def size(ref):
        return math.prod(ref.shape) * 2

    def slot_of(name):
        if name not in names:
            names[name] = len(names)
        return names[name]

    def send(src, dst, name, dev, sem=0, count=1):
        assert size(src) % UNIT == 0
        sent[sem] += count * (size(src) // UNIT)
        pltpu.make_async_remote_copy(
            src_ref=src, dst_ref=dst, send_sem=ssem.at[sem], recv_sem=rsem.at[slot_of(name)],
            device_id=dev, device_id_type=MESH,
        ).start()

    def wait(dst, name):
        pltpu.make_async_remote_copy(
            src_ref=dst, dst_ref=dst, send_sem=ssem.at[0], recv_sem=rsem.at[slot_of(name)],
            device_id=mate, device_id_type=MESH,
        ).wait_recv()

    phase("start")
    barrier = pltpu.get_barrier_semaphore()
    peers = [mate] + [yat(k) for k in range(1, NY)] + [xat(k) for k in range(1, NX)]
    peers += [zat(k) for k in range(1, NZ)]
    for dev in peers:
        pl.semaphore_signal(barrier, inc=1, device_id=dev, device_id_type=MESH)

    loads = {}
    for k, (name, src, dst) in enumerate(
        (
            ("tr", tr_hbm, tr), ("og", og_hbm, og), ("gn", gain_hbm, gn), ("sr", sr_hbm, sg.at[c, 0]),
            ("of", off_hbm, of), ("sv", saved_hbm, sv),
            ("q", wq_hbm, wq), ("o", wo_hbm, wo), ("k", wk_hbm, wk), ("v", wv_hbm, wv),
        )
    ):
        loads[name] = pltpu.make_async_copy(src, dst, lsem.at[k])
        loads[name].start()

    for name in ("tr", "og", "gn"):
        loads[name].wait()
    gain = gn[...].astype(F32)
    gain = jnp.concatenate([gain[s : s + 1] for s in range(16)], axis=1)
    target = tr[...].astype(F32)
    inverse = lax.rsqrt(jnp.mean(target * target, axis=1, keepdims=True) + EPSILON)
    normed = target * inverse * gain
    tg[c, y] = jnp.concatenate([normed, og[...].astype(F32)], axis=0).astype(BF16)
    for f in range(NZ):
        nzs[f] = normed[:, 256 * f : 256 * f + 256].astype(BF16)
    for f in range(NX):
        nxs[f] = jnp.concatenate(
            [normed[:, 256 * g + 64 * f : 256 * g + 64 * f + 64] for g in range(NZ)], axis=1
        ).astype(BF16)
    phase("barrier")
    pl.semaphore_wait(barrier, len(peers))

    phase("tgwait")
    loads["sr"].wait()
    send(sg.at[c, 0], sg.at[c, 0], ("sg0",), mate)

    def tg_of(k):
        return tg.at[c, (y + NY - k) % NY]

    for k in (4, 3, 5, 2, 6, 1, 7):
        send(tg_of(0), tg_of(0), ("tg", k), yat(k))
    send(tg_of(0), tg_of(0), ("tgm",), mate)
    for k in range(1, NZ):
        send(nzs.at[(z + k) % NZ], nza.at[k], ("nza",), zat(k))
    for e in range(1, NX):
        send(nxs.at[(x + e) % NX], nxa.at[x], ("nxa",), xat(e))
    for k in (3, 5, 2, 6, 4, 1, 7):
        wait(tg_of(k), ("tg", k))
        send(tg_of(k), tg_of(k), ("tgm",), mate)

    @pl.when(c == 1)
    def _():
        wait(sg.at[0, 0], ("sg0",))
        for k in (2, 6, 1, 7):
            send(sg.at[:, 0], sg.at[:, k], ("sg", k), yat(k), 1)

    phase("tgmate")
    wait(tg.at[1 - c], ("tgm",))

    phase("qproj")
    for s in range(16):
        rows = tg[s % 2, s // 2].astype(F32)
        xn[4 * s : 4 * s + 4] = rows[0:4]
        xo[4 * s : 4 * s + 4] = rows[4:8]
    loads["o"].wait()
    hgrad = nt(xo[...].astype(BF16), wo[...]).astype(BF16)
    xf[0, x] = hgrad
    for e in (2, 1, 3):
        send(xf.at[0, x], xf.at[0, x], ("xfx", e), xat(e))
    loads["q"].wait()
    zf[0, x, 0:64] = nn(xn[...].astype(BF16), wq[...]).astype(BF16)
    loads["sv"].wait()
    loads["of"].wait()
    deltas = jnp.sum(hgrad.astype(F32) * sv[...].astype(F32), axis=1, keepdims=True)
    deltas = jnp.broadcast_to(deltas, (64, 128)).T[0:16]
    first = lax.broadcasted_iota(jnp.int32, (16, 64), 0) == 0
    both = jnp.where(first, of[...].astype(F32), deltas).astype(BF16)
    place = lax.broadcasted_iota(jnp.int32, (64, 256), 1) == x * 64 + lax.broadcasted_iota(
        jnp.int32, (64, 256), 0
    )
    zf[0, x, 64:72] = nn(both, place.astype(F32).astype(BF16))[0:8].astype(BF16)

    def xs(e):
        return (x + NX - e) % NX

    def zf_x(k):
        for e in (2, 1, 3):
            send(zf.at[k, x], zf.at[k, x], ("zfx", k, e), xat(e))

    def zf_z(k):
        if k:
            wait(zf.at[k, x], ("zfz", k))
        if k <= 3:
            send(zf.at[k, x], zf.at[k + 1, x], ("zfz", k + 1), zat(1))
        if k == 0 or k >= 6:
            send(zf.at[k, x], zf.at[(k - 1) % NZ, x], ("zfz", (k - 1) % NZ), zat(7))

    def zf_end(k):
        for e in (1, 3, 2):
            wait(zf.at[k, xs(e)], ("zfx", k, e))

    def xf_z(k, e):
        if k:
            wait(xf.at[k, xs(e)], ("xfz", k, e))
        if k <= 2 or (k == 3 and e % 2 == 0):
            send(xf.at[k, xs(e)], xf.at[k + 1, xs(e)], ("xfz", k + 1, e), zat(1))
        if k == 0 or k >= 6 or (k == 5 and e % 2 == 1):
            send(xf.at[k, xs(e)], xf.at[(k - 1) % NZ, xs(e)], ("xfz", (k - 1) % NZ, e), zat(7))

    def sg_in(*ks):
        @pl.when(c == 1)
        def _():
            for k in ks:
                wait(sg.at[:, k], ("sg", k))
                if k == 2:
                    send(sg.at[:, 2], sg.at[:, 3], ("sg", 3), yat(1), 1)
                    send(sg.at[0, 2], sg.at[0, 4], ("sg", 4), yat(2), 1)
                if k == 6:
                    send(sg.at[:, 6], sg.at[:, 5], ("sg", 5), yat(7), 1)
                    send(sg.at[1, 6], sg.at[1, 4], ("sg", 4), yat(6), 1)
                send(sg.at[:, k], sg.at[:, k], ("sgm",), mate, 1)

    back = {2: 3, 6: 1}

    def x_sends(k):
        e = back.get(k)
        if e is None:
            for e in (2, 1, 3):
                send(part.at[k, (x + e) % NX], xin.at[k, e - 1], ("xin", k), xat(e))
        else:
            send(part.at[k, (x + 2) % NX], reli.at[k // 4], ("rel", k), xat(e))
            send(part.at[k, (x + 4 - e) % NX], xin.at[k, 1], ("xin", k), xat(4 - e))

    def x_relay(k):
        e = back[k]
        n = k // 4
        wait(reli.at[n], ("rel", k))
        relo[n] = (part[k, (x + e) % NX].astype(F32) + reli[n].astype(F32)).astype(BF16)
        send(relo.at[n], xin.at[k, 0], ("xin", k), xat(e))

    def x_sum(k):
        count = 2 if k in back else 3
        wait(xin.at[k, 0:count], ("xin", k))
        total = part[k, x].astype(F32)
        for n in range(count):
            total += xin[k, n].astype(F32)
        return total

    def z_send(k):
        if k:
            zout[k] = x_sum(k).astype(BF16)
            send(zout.at[k], zin.at[k], ("zin",), zat(NZ - k))

    def group(k, first):
        q = zf[k, :, 0:64, :].reshape(256, 256)
        h = xf[k].reshape(256, 256)
        stat = jnp.sum(zf[k, :, 64:72, :].astype(F32), axis=0)
        score = nt(kb[...], q)
        prob = jnp.exp(score * SCALE - (SHIFT + stat[0:1]))
        grad = prob * (nt(vb[...], h) - stat[1:2]) * SCALE
        prob = prob.astype(BF16)
        dv_new = nn(prob, h)
        dk_new = nn(grad.astype(BF16), q)
        if first:
            dv[...] = dv_new
            dk[...] = dk_new
        else:
            dv[...] += dv_new
            dk[...] += dk_new
        dq = nn(jnp.transpose(grad).astype(BF16), kb[...])
        part[k] = dq.astype(BF16).reshape(4, 64, 256)

    def work(k, first=False):
        phase(f"group{k}")
        zf_end(k)
        group(k, first)
        if k not in (0, 1, 7):
            x_sends(k)

    phase("spsend")
    zf_z(0)
    xf_z(0, 0)
    zf_x(0)

    phase("step1")
    for e in (1, 3):
        wait(xf.at[0, xs(e)], ("xfx", e))
        xf_z(0, e)
    for k in (1, 7):
        zf_z(k)
    sg_in(2, 6)
    wait(xf.at[0, xs(2)], ("xfx", 2))
    xf_z(0, 2)
    for k in (1, 7):
        xf_z(k, 0)
    for k in (1, 7):
        zf_x(k)
    phase("step2")
    for e in (1, 3):
        xf_z(1, e)
        xf_z(7, e)
    for k in (2, 6):
        zf_z(k)
        xf_z(k, 0)
    for k in (1, 7):
        xf_z(k, 2)
    for k in (2, 6):
        zf_x(k)
    sg_in(1, 7, 3, 5, 4)
    nza[0] = nzs[z]
    wait(nza.at[1:8], ("nza",))
    nyb[c, y] = nza[...]
    nxa[x] = nxs[x]
    wait(nxa.at[0:3], ("nxa",))
    nyx[c, y] = nxa[...]
    for k in (4, 3, 5, 2, 6, 1, 7):
        send(nza, nyb.at[c, y], ("nyb",), yat(k))
    send(nza, nyb.at[c, y], ("nybm",), mate)
    for k in (4, 3, 5, 2, 6, 1, 7):
        send(nxa, nyx.at[c, y], ("nyx",), yat(k))
    send(nxa, nyx.at[c, y], ("nyxm",), mate)
    phase("kproj")

    @pl.when(c == 0)
    def _():
        wait(sg.at[1, 0], ("sg0",))
        wait(sg.at[:, 1:8], ("sgm",))

    loads["k"].wait()
    kb[...] = nn(sg[...].reshape(256, 2048), wk[...]).astype(BF16)
    phase("vproj")
    loads["v"].wait()
    vb[...] = nn(sg[...].reshape(256, 2048), wv[...]).astype(BF16)
    phase("step3")
    for e in (1, 3):
        xf_z(2, e)
        xf_z(6, e)
    for k in (3, 5):
        zf_z(k)
        xf_z(k, 0)
    for k in (2, 6):
        xf_z(k, 2)
    for k in (3, 5):
        zf_x(k)
    work(1, True)
    work(7)
    phase("step4")
    for e in (1, 3):
        xf_z(3, e)
        xf_z(5, e)
    zf_z(4)
    zf_x(4)
    for k in (3, 5):
        xf_z(k, 2)
    for k in (1, 7):
        send(part.at[k], near.at[k // 7], ("near", k), zat(NZ - k))
    work(2)
    work(6)
    work(0)
    phase("xf4")
    for e in range(4):
        xf_z(4, e)
    work(3)
    work(5)
    work(4)
    x_relay(2)
    x_relay(6)

    def gsum_stage(count):
        wait(gin, ("gm",))
        for k in (4, 3, 5, 1, 7):
            gsum[k] = (gout[c, k].astype(F32) + gin[k].astype(F32)).astype(BF16)
        send(gsum.at[4], gmid.at[2], ("gmid",), yat((NY - 2 * way) % NY), count=count)
        send(gsum.at[3], gmid.at[0], ("gmid",), yat(7), count=count)
        send(gsum.at[5], gmid.at[1], ("gmid",), yat(1), count=count)
        send(gsum.at[1], grecv.at[1], ("g",), yat(7), count=count)
        send(gsum.at[7], grecv.at[7], ("g",), yat(1), count=count)

    phase("gmat1")
    dkb = dk[...].astype(BF16)
    dvb = dv[...].astype(BF16)

    def gmat(half):
        lo = 128 * half
        for f in range(4):
            cols = pl.ds(512 * f, 512)
            gout[half, :, :, cols] = (
                (nt(dkb[lo : lo + 128], wk[cols, :]) + nt(dvb[lo : lo + 128], wv[cols, :]))
                .astype(BF16)
                .reshape(8, 16, 512)
            )

    gmat(0)
    phase("gmat0")
    gmat(1)
    send(gout.at[1 - c], gin, ("gm",), mate)
    phase("nyb")
    wait(nyb.at[0, 0:7], ("nyb",))
    for k in range(1, NY):
        send(nyb.at[c, (y + k) % NY], nyb.at[c, (y + k) % NY], ("nybm",), mate)
    wait(nyx.at[0, 0:7], ("nyx",))
    for k in range(1, NY):
        send(nyx.at[c, (y + k) % NY], nyx.at[c, (y + k) % NY], ("nyxm",), mate)
    phase("near")
    wait(near.at[0], ("near", 1))
    wait(near.at[1], ("near", 7))
    part[0] = (part[0].astype(F32) + near[0].astype(F32) + near[1].astype(F32)).astype(BF16)
    x_sends(0)
    phase("gsumS")
    pl.when(c == 0)(functools.partial(gsum_stage, 1))
    phase("zsend3")
    z_send(3)
    phase("zsend5")
    z_send(5)
    phase("zsend4")
    z_send(4)
    phase("zsend2")
    z_send(2)
    phase("zsend6")
    z_send(6)
    phase("nrt")
    wait(nyb.at[0], ("nybm",))
    for s in range(16):
        rows = nyb[s % 2, s // 2].astype(F32)
        for k in range(NZ):
            nr[k, 4 * s : 4 * s + 4] = rows[k]
    for j in range(4):
        pair = nr[2 * j : 2 * j + 2].reshape(128, 256)
        nrt[:, 128 * j : 128 * j + 128] = pair.T.astype(BF16)
    wait(nyx.at[0], ("nyxm",))
    for s in range(16):
        rows = nyx[s % 2, s // 2].astype(F32)
        for k in range(NX):
            nrx[k, 4 * s : 4 * s + 4] = rows[k]
    for j in range(2):
        pair = nrx[2 * j : 2 * j + 2].reshape(128, 512)
        nrtx[:, 128 * j : 128 * j + 128] = pair.T.astype(BF16)
    phase("gsumN")
    pl.when(c == 1)(functools.partial(gsum_stage, 0))
    phase("qflat")
    total = x_sum(0)
    wait(zin.at[2:7], ("zin",))
    for k in range(2, 7):
        total += zin[k].astype(F32)
    qflat = total.astype(BF16)
    qz[0] = qflat[:, 0:128]
    qx[x] = qflat[:, 128:256]
    for e in (2, 1, 3):
        send(qx.at[x], qx.at[x], ("qx",), xat(e))
    for k in (4, 3, 5, 2, 6, 1, 7):
        send(qz.at[0], qz.at[k], ("qz",), zat(k))

    phase("ng")
    for f in range(2):
        halves = [nt(qflat, wq[1024 * g + 512 * f : 1024 * g + 512 * f + 512, :]) for g in range(2)]
        for s in range(16):
            nout[s % 2, s // 2, :, 512 * f : 512 * f + 512] = jnp.concatenate(
                [half[4 * s : 4 * s + 4] for half in halves], axis=0
            ).astype(BF16)
    send(nout.at[1 - c], nin, ("nm",), mate)
    phase("gmid")
    wait(gmid, ("gmid",))
    for k, n in ((2, 0), (6, 1)):
        mid = jnp.where(c == n, gmid[2].astype(F32), 0.0) + gmid[n].astype(F32)
        gsum[k] = (gout[c, k].astype(F32) + gin[k].astype(F32) + mid).astype(BF16)
        send(gsum.at[k], grecv.at[k], ("g",), yat(NY - k))
    phase("nsum")
    wait(nin, ("nm",))
    nsum[...] = (nout[c].astype(F32) + nin[...].astype(F32)).astype(BF16)
    for k in (4, 3, 5, 2, 6, 1, 7):
        send(nsum.at[(y + NY - k) % NY], nrecv.at[k], ("n",), yat(NY - k))

    phase("wmat2")
    wait(qx.at[0:3], ("qx",))
    wz[...] = nn(nrtx[...], qx[...].reshape(256, 128)).astype(BF16).reshape(8, 64, 128)
    for k in (4, 3, 5, 2, 6, 1, 7):
        send(wz.at[(z + k) % NZ], wzin.at[k], ("wz",), zat(k))
    phase("wmat")
    wait(qz.at[1:8], ("qz",))
    wpart[...] = nn(nrt[...], qz[...].reshape(512, 128)).astype(BF16).reshape(4, 64, 128)
    for e in (2, 1, 3):
        send(wpart.at[(x + e) % NX], win.at[e], ("w",), xat(e))

    phase("gfin")
    wait(grecv.at[0:4], ("g",))
    total = gout[c, 0].astype(F32) + gin[0].astype(F32)
    for k in (1, 2, 6, 7):
        total += grecv[k].astype(F32)
    sgrad_ref[...] = total

    phase("nfin")
    wait(nrecv.at[1:8], ("n",))
    total = nsum[y].astype(F32)
    for k in range(1, NY):
        total += nrecv[k].astype(F32)
    scaled = jnp.concatenate([total[0:4], total[4:8]], axis=1) * gain
    mean = jnp.mean(scaled * target, axis=1, keepdims=True)
    tgrad_ref[...] = inverse * scaled - target * (inverse * inverse * inverse) * mean

    phase("wfin")
    wait(win.at[1:4], ("w",))
    total = wpart[x].astype(F32)
    for e in range(1, NX):
        total += win[e].astype(F32)
    wgrad_ref[:, 0:128] = total
    wait(wzin.at[1:8], ("wz",))
    total = wz[z].astype(F32)
    for k in range(1, NZ):
        total += wzin[k].astype(F32)
    wgrad_ref[:, 128:256] = total

    phase("sendwait")
    def sent_all(sem):
        whole = units.at[0 : sent[sem]]
        pltpu.make_async_remote_copy(
            src_ref=whole, dst_ref=whole, send_sem=ssem.at[sem], recv_sem=rsem.at[0],
            device_id=mate, device_id_type=MESH,
        ).wait_send()

    sent_all(0)

    @pl.when(c == 1)
    def _():
        sent_all(1)

    phase(None)
    assert max(sent) <= UNITS and len(names) <= RECVS, (sent[0], len(names))


def finish(a_ref, b_ref, c_ref, oa_ref, ob_ref, oc_ref):
    oa_ref[...] = a_ref[...]
    ob_ref[...] = b_ref[...]
    oc_ref[...] = c_ref[...]


def body(tr, sr, gain, wq, wk, wv, wo, saved, offset, og):
    vm = pl.BlockSpec(memory_space=pltpu.VMEM)
    hb = pl.BlockSpec(memory_space=pl.ANY)

    def buf(*shape, dtype=BF16):
        return pltpu.VMEM(shape, dtype)

    outs = (
        jax.ShapeDtypeStruct((4, 2048), F32),
        jax.ShapeDtypeStruct((16, 2048), F32),
        jax.ShapeDtypeStruct((64, 256), F32),
    )
    results = pl.pallas_call(
        kernel,
        out_shape=tuple(pltpu.VMEM(o.shape, o.dtype) for o in outs),
        in_specs=[hb] * 10,
        out_specs=(vm, vm, vm),
        scratch_shapes=[
            buf(4, 2048), buf(16, 128), buf(64, 256), buf(1, 64), buf(4, 2048),
            buf(2, 8, 8, 2048), buf(64, 2048, dtype=F32), buf(64, 2048, dtype=F32),
            buf(8, 4, 256), buf(8, 4, 256), buf(2, 8, 8, 4, 256),
            buf(8, 64, 256, dtype=F32), buf(256, 512),
            buf(4, 4, 512), buf(4, 4, 512), buf(2, 8, 4, 4, 512), buf(4, 64, 512, dtype=F32), buf(512, 256),
            buf(2, 8, 16, 2048),
            buf(2048, 256), buf(2048, 256), buf(2048, 256), buf(256, 2048),
            buf(8, 4, 72, 256), buf(8, 4, 64, 256),
            buf(256, 256), buf(256, 256),
            buf(256, 256, dtype=F32), buf(256, 256, dtype=F32),
            buf(8, 4, 64, 256), buf(2, 4, 64, 256), buf(2, 64, 256), buf(2, 64, 256),
            buf(8, 3, 64, 256),
            buf(8, 64, 256), buf(8, 64, 256),
            buf(8, 64, 128), buf(4, 64, 128), buf(8, 64, 128), buf(8, 64, 128), buf(4, 64, 128), buf(4, 64, 128),
            buf(2, 8, 16, 2048), buf(8, 16, 2048), buf(8, 16, 2048), buf(3, 16, 2048), buf(8, 16, 2048),
            buf(2, 8, 8, 1024), buf(8, 8, 1024), buf(8, 8, 1024), buf(8, 8, 1024),
            buf(UNITS, 4, 256),
            pltpu.SemaphoreType.DMA((2,)),
            pltpu.SemaphoreType.DMA((RECVS,)),
            pltpu.SemaphoreType.DMA((10,)),
        ],
        compiler_params=pltpu.CompilerParams(
            collective_id=0, has_side_effects=True, vmem_limit_bytes=60 * 1024 * 1024
        ),
    )(tr, sr, gain.reshape(16, 128), wq, wk, wv, wo, saved, offset.reshape(1, 64), og)
    return pl.pallas_call(
        finish, out_shape=outs, in_specs=[vm, vm, vm], out_specs=(vm, vm, vm)
    )(*[pltpu.with_memory_space_constraint(r, pltpu.VMEM) for r in results])


def solution(mesh):
    split = Mesh(mesh.devices.reshape(NZ, NX, mesh.shape["tp"]), ("sp_0", "sp_1", "tp"))
    placed = (
        P(SP_TP, None), P(SP_TP, None), P(), P(None, "tp"), P(None, "tp"), P(None, "tp"),
        P("tp", None), P(SP, "tp"), P(SP, "tp"), P(SP_TP, None),
    )
    return jax.shard_map(
        body,
        mesh=split,
        in_specs=placed,
        out_specs=(P(SP_TP, None), P(SP_TP, None), P(SP, "tp")),
        check_vma=False,
    )
```
